256 devices in a mesh: sp: 64 (over z, x, core), tp: 4 (over y).
Axes of the slice: x: 4, y: 4, z: 8, core: 2. Of those that a mesh axis runs over, the one named last changes fastest.
Arguments:
- queries: bfloat16 [40960, 1024], P('sp', 'tp'), may hold values from -160 to 160
- keys: bfloat16 [40960, 256], P('sp', 'tp'), may hold values from -24 to 24
- values: bfloat16 [40960, 256], P('sp', 'tp'), may hold values from -6 to 6
- documents: int32 [40960], P('sp'), may hold values from 0 to 15, never falling along the last dimension, each value on 1 to 5120 neighbouring positions
- sinks: float32 [16], P('tp'), may hold values from -1 to 4
- out_weight: bfloat16 [1024, 2048], replicated, may hold values from -0.1875 to 0.1875
- residual: bfloat16 [40960, 2048], P(('sp', 'tp')), may hold values from -3 to 3
- norm_gain: float32 [2048], replicated, may hold values from 0.1 to 1.9
- up_weight: bfloat16 [2048, 8192], P('sp', 'tp'), may hold values from -0.125 to 0.125
- down_weight: bfloat16 [8192, 2048], P('tp', 'sp'), may hold values from -0.0625 to 0.0625
Outputs:
- layer_out: bfloat16 [40960, 2048], P(('sp', 'tp'))
The draws below stay inside these ranges and needn't reach their ends.
Inputs may be any that keep to these rules, and one draw needn't show every extreme that they name: `documents`: document numbers never fall along the positions; each document holds at most 5120 positions.
All inputs are finite; a program needn't handle non-finite values.
Results may differ from the reference program's by a relative error of at most 0.0095.
Values may be sent and summed in bfloat16 or wider, within the bound.
A program may use at most 64 MiB of HBM per device.

```python
import math
import jax
import jax.numpy as jnp
import numpy as np
from jax import lax

D = 2048
QUERY_HEADS = 16
KEY_VALUE_HEADS = 4
HEAD_SIZE = 64
FF = 8192
WINDOW_REACH = 128
TOK_DEV = 640
PACK_TOKENS = 40960
ATTN = 1024
FF_DEV = 2048
DOCS = 16
N_SP = 64
N_TP = 4


def drawn(key):
    starting_keys = jax.random.normal(jax.random.fold_in(key, 11), (PACK_TOKENS, KEY_VALUE_HEADS, HEAD_SIZE), jnp.float32)
    base_queries = jax.random.normal(jax.random.fold_in(key, 12), (PACK_TOKENS, QUERY_HEADS, HEAD_SIZE), jnp.float32)
    output_keys = starting_keys
    output_queries = base_queries
    return (output_queries.reshape(PACK_TOKENS, QUERY_HEADS * HEAD_SIZE).astype(jnp.bfloat16), output_keys.reshape(PACK_TOKENS, KEY_VALUE_HEADS * HEAD_SIZE).astype(jnp.bfloat16))


def draw_queries(key, part):
    return drawn(key)[0]


def draw_keys(key, part):
    return drawn(key)[1]


def shard_levels(stream_key, dims, cuts, low, largest):
    level = 1.0
    for dim, blocks in cuts:
        heights = jax.random.uniform(jax.random.fold_in(jax.random.fold_in(stream_key, 6), dim), (blocks,), jnp.float32, low / len(cuts), largest / len(cuts))
        level = level * jnp.repeat(jnp.exp(heights), dims[dim] // blocks).reshape((-1,) + (1,) * (len(dims) - 1 - dim))
    return level


def split_up(count, total, limit, lean):
    loads = [(1 << 20) // math.isqrt(grade ** lean) + 1 for grade in range(2, count + 1)]
    surplus, counts = total - limit - (count - 1), [1] * (count - 1)
    while surplus > 0:
        free = [i for i in range(count - 1) if counts[i] < limit]
        mass, budget = sum([loads[i] for i in free]), surplus
        for i in free:
            more = min(limit - counts[i], max(1, budget * loads[i] // mass), surplus)
            counts[i] = counts[i] + more
            surplus = surplus - more
    return np.array([limit] + counts)


def ragged(rng, amount, total, limit, lean):
    if amount == 2:
        one = jax.random.randint(rng, (), max(1, total - limit), min(limit, total - 1) + 1)
        return jnp.stack([one, total - one])
    lengths = jnp.asarray(split_up(amount, total, limit, lean), jnp.int32)
    couples = (amount - 1) // 2
    giver, taker = lengths[1:1 + 2 * couples:2], lengths[2:2 + 2 * couples:2]
    margin = jnp.minimum(giver - 1, limit - taker)
    shifted = jax.random.randint(jax.random.fold_in(rng, 1), (couples,), 0, 1 << 20) % (margin + 1)
    lengths = lengths.at[1:1 + 2 * couples:2].set(giver - shifted).at[2:2 + 2 * couples:2].set(taker + shifted)
    return lengths[jax.random.permutation(jax.random.fold_in(rng, 2), amount)]


def noise(own_key, shape, spread, bound, pieces=(), kind=jnp.bfloat16):
    array = jax.random.normal(own_key, shape, jnp.float32) * spread
    if len(pieces) > 0:
        array = shard_levels(own_key, shape, pieces, -0.22, 0.18) * array
    return jnp.clip(array, min=-bound, max=bound).astype(kind)


def setup_inputs(seed: int = 0) -> dict:
    streams_of = jax.random.split(jax.random.key(seed), 11)
    queries = draw_queries(jax.random.fold_in(streams_of[10], 71), 0)
    keys = draw_keys(jax.random.fold_in(streams_of[10], 71), 0)
    values = noise(streams_of[2], (PACK_TOKENS, KEY_VALUE_HEADS * HEAD_SIZE), 1.0, 6.0, ((0, 64), (1, 4)))
    documents = jnp.searchsorted(jnp.cumsum(ragged(streams_of[3], DOCS, PACK_TOKENS, 8 * TOK_DEV, 1)), jnp.arange(PACK_TOKENS), side="right").astype(jnp.int32)
    sinks = jnp.clip(-1.0 + 5.0 * jax.random.uniform(streams_of[4], (QUERY_HEADS,), jnp.float32) ** shard_levels(streams_of[4], (QUERY_HEADS,), ((0, 4),), -0.2, 0.2), -1.0, 4.0)
    out_weight = noise(streams_of[5], (ATTN, D), ATTN ** -0.5, 0.1875)
    residual = noise(streams_of[6], (PACK_TOKENS, D), 0.5, 3.0, ((0, 256),))
    norm_gain = jnp.clip(1.0 + 0.18 * jax.random.normal(streams_of[7], (D,), jnp.float32), 0.1, 1.9)
    up_weight = noise(streams_of[8], (D, FF), D ** -0.5, 0.125, ((0, 64), (1, 4)))
    down_weight = noise(streams_of[9], (FF, D), FF ** -0.5, 0.0625, ((0, 4), (1, 64)))
    return {"queries": queries, "keys": keys, "values": values, "documents": documents, "sinks": sinks, "out_weight": out_weight, "residual": residual, "norm_gain": norm_gain, "up_weight": up_weight, "down_weight": down_weight}


masked_score = -1e+30
epsilon = 1e-06

def rounded(value):
    return lax.optimization_barrier(value.astype(jnp.bfloat16))

def reference(queries, keys, values, documents, sinks, out_weight, residual, norm_gain, up_weight, down_weight):
    query_group = QUERY_HEADS // KEY_VALUE_HEADS
    block_list = PACK_TOKENS // WINDOW_REACH
    key_matrix = jnp.concatenate([jnp.zeros((WINDOW_REACH, KEY_VALUE_HEADS * HEAD_SIZE), jnp.bfloat16), keys], axis=0).reshape(block_list + 1, WINDOW_REACH, KEY_VALUE_HEADS, HEAD_SIZE)
    value_matrix = jnp.concatenate([jnp.zeros((WINDOW_REACH, KEY_VALUE_HEADS * HEAD_SIZE), jnp.bfloat16), values], axis=0).reshape(block_list + 1, WINDOW_REACH, KEY_VALUE_HEADS, HEAD_SIZE)
    doc_ids = documents.astype(jnp.int32)
    key_docs = jnp.concatenate([jnp.full((WINDOW_REACH,), -1, jnp.int32), doc_ids], axis=0).reshape(block_list + 1, WINDOW_REACH)
    query_docs = doc_ids.reshape(block_list, WINDOW_REACH)
    grouped_queries = queries.reshape(block_list, WINDOW_REACH, KEY_VALUE_HEADS, query_group, HEAD_SIZE)
    head_sink_logit = sinks.astype(jnp.float32).reshape(KEY_VALUE_HEADS, query_group, 1)
    row_index = jnp.arange(WINDOW_REACH, dtype=jnp.int32)[:, None]
    col_index = jnp.arange(2 * WINDOW_REACH, dtype=jnp.int32)[None, :]
    distance = WINDOW_REACH + row_index - col_index
    near = (distance >= 0) & (distance < WINDOW_REACH)

    def one_block(items):
        block_queries, early_keys, late_keys, early_values, late_values, early_docs, late_docs, own_docs = items
        band_keys = jnp.concatenate([early_keys, late_keys], axis=0).astype(jnp.float32)
        band_values = jnp.concatenate([early_values, late_values], axis=0).astype(jnp.float32)
        band_docs = jnp.concatenate([early_docs, late_docs], axis=0)
        visible = (near & (band_docs[None, :] == own_docs[:, None]))[None, None]
        scores = jnp.einsum('qhgd,shd->hgqs', block_queries.astype(jnp.float32), band_keys) * HEAD_SIZE ** (-0.5)
        scores = jnp.where(visible, scores, masked_score)
        top = jnp.maximum(lax.optimization_barrier(jnp.max(scores, axis=-1)), head_sink_logit)
        exponent = jnp.where(visible, jnp.exp(scores - top[..., None]), 0.0)
        total = jnp.exp(head_sink_logit - top) + lax.optimization_barrier(jnp.sum(exponent, axis=-1))
        shares = rounded(exponent / total[..., None])
        attended = jnp.einsum('hgqs,shd->qhgd', shares.astype(jnp.float32), band_values)
        return attended.astype(jnp.bfloat16).reshape(WINDOW_REACH, QUERY_HEADS * HEAD_SIZE)
    attended = lax.map(one_block, (grouped_queries, key_matrix[:-1], key_matrix[1:], value_matrix[:-1], value_matrix[1:], key_docs[:-1], key_docs[1:], query_docs))
    attended = attended.reshape(PACK_TOKENS, QUERY_HEADS * HEAD_SIZE)
    projected = jnp.dot(attended.astype(jnp.float32), out_weight.astype(jnp.float32), preferred_element_type=jnp.float32)
    mixed = rounded(residual.astype(jnp.float32) + rounded(projected).astype(jnp.float32))
    widened = mixed.astype(jnp.float32)
    normed = (widened * lax.rsqrt(lax.optimization_barrier(jnp.mean(widened * widened, axis=-1, keepdims=True)) + epsilon) * norm_gain.astype(jnp.float32)).astype(jnp.bfloat16)
    down_groups = down_weight.astype(jnp.float32).reshape(N_TP, FF_DEV, D)

    def mixer_block(rows):
        before = jnp.dot(rows.astype(jnp.float32), up_weight.astype(jnp.float32), preferred_element_type=jnp.float32)
        hidden = jnp.square(jax.nn.relu(before)).astype(jnp.bfloat16)
        parts = jnp.einsum('rnf,nfd->nrd', hidden.reshape(rows.shape[0], N_TP, FF_DEV).astype(jnp.float32), down_groups)
        return lax.optimization_barrier(jnp.sum(rounded(parts).astype(jnp.float32), axis=0))
    branch = lax.map(mixer_block, normed.reshape(N_SP, TOK_DEV, D)).reshape(PACK_TOKENS, D)
    return (widened + rounded(branch).astype(jnp.float32)).astype(jnp.bfloat16)
```

```python
import functools
import heapq

import jax
import jax.numpy as jnp
from jax import lax
from jax.experimental import pallas as pl
from jax.experimental.pallas import tpu as pltpu
from jax.sharding import PartitionSpec as P

MESH = pl.DeviceIdType.MESH
NZ, NX, NY = 8, 4, 4
HEAD = 64
REACH = 128
TOK = 640
OWN = 160
HALF = 80
D = 2048
SHARD = 32
masked_score = -1e30
epsilon = 1e-06

STREAMS = ((0, "z", 0, D), (1, "x", 0, D))
RATE = 46.6e3
LATENCY = 1.8
DZ_ORDER = (0, 1, -1, 2, -2, 3, -3, 4)


def onward(item):
    s, dz, dx, part = item
    mode = STREAMS[s][1]
    out = []

    def along_z():
        if dz == 0:
            out.append(("z", 1, (s, 1, dx, None)))
            out.append(("z", -1, (s, -1, dx, None)))
        elif dz in (1, 2):
            out.append(("z", 1, (s, dz + 1, dx, None)))
        elif dz in (-1, -2):
            out.append(("z", -1, (s, dz - 1, dx, None)))
        elif dz == 3:
            out.append(("z", 1, (s, 4, dx, 0)))
        elif dz == -3:
            out.append(("z", -1, (s, 4, dx, 1)))

    def along_x():
        if dx == 0:
            out.append(("x", 1, (s, dz, 1, part)))
            out.append(("x", -1, (s, dz, -1, part)))
        elif dx == 1:
            if dz == 0:
                out.append(("x", 1, (s, dz, 2, 0)))
            elif dz in (1, -2, 3) or (dz == 4 and part == 0):
                out.append(("x", 1, (s, dz, 2, part)))
        elif dx == -1:
            if dz == 0:
                out.append(("x", -1, (s, dz, 2, 1)))
            elif dz in (-1, 2, -3) or (dz == 4 and part == 1):
                out.append(("x", -1, (s, dz, 2, part)))

    if mode == "z":
        if dx == 0:
            along_z()
        along_x()
    else:
        if dz == 0:
            along_x()
        if part is None or dz != 0:
            if part is None:
                along_z()
        elif part == 1:
            along_z()
    return out


def plan():
    free = {}
    heap = []

    def put(now, item):
        for axis, way, there in onward(item):
            size = SHARD * STREAMS[there[0]][3] * 2
            if there[3] is not None:
                size //= 2
            begin = max(now, free.get((axis, way), 0.0))
            end = begin + size / RATE
            free[(axis, way)] = end
            heapq.heappush(heap, (end + LATENCY, str(there), there))

    for s in range(len(STREAMS)):
        put(0.0, (s, 0, 0, None))
    order = []
    while heap:
        now, _, item = heapq.heappop(heap)
        order.append((now, item))
        put(now, item)
    return order


PLAN = plan()
SLOT = {item: k for k, (_, item) in enumerate(PLAN)}


def kernel(
    q_ref, k_ref, v_ref, docs_ref, sink_ref, w_hbm, res_hbm, gain_ref, up_ref, down_ref,
    out_ref,
    up_all, down_all, w_ref, res_ref, k_band, v_band, k_prev, v_prev, docs_prev, docs_band,
    attended, heads, mixed, normed, hidden, parts, first_a, first_b, last_a, last_b,
    arrive, send_sems, twin_sem, twin_arrive, load_sem, halo_sem, halo_send,
    swap_sem, swap_send, row_sem, row_send, sum_sem, sum_send, end_sem,
):
    sp = lax.axis_index("sp")
    y = lax.axis_index("tp")
    c = lax.rem(sp, 2)
    x = lax.rem(sp // 2, NX)
    z = sp // (2 * NX)

    def place(zz, xx, cc):
        return (zz * NX + xx) * 2 + cc

    def near(axis, way):
        if axis == "z":
            return {"sp": place(lax.rem(z + way + NZ, NZ), x, c), "tp": y}
        return {"sp": place(z, lax.rem(x + way + NX, NX), c), "tp": y}

    twin = {"sp": place(z, x, 1 - c), "tp": y}

    def column(by):
        return {"sp": sp, "tp": lax.rem(y + by + NY, NY)}

    def line(by):
        return {"sp": lax.rem(sp + by + 2 * NX * NZ, 2 * NX * NZ), "tp": y}

    w_load = pltpu.make_async_copy(w_hbm, w_ref, load_sem.at[0])
    res_load = pltpu.make_async_copy(res_hbm, res_ref, load_sem.at[1])
    w_load.start()
    res_load.start()

    barrier = pltpu.get_barrier_semaphore()
    greeted = [near("z", 1), near("z", -1), near("x", 1), near("x", -1), twin,
               column(1), column(2), column(3), line(1), line(-1)]
    for device in greeted:
        pl.semaphore_signal(barrier, inc=1, device_id=device, device_id_type=MESH)
    pl.semaphore_wait(barrier, len(greeted))

    def remote(src, dst, send, recv, device):
        return pltpu.make_async_remote_copy(
            src_ref=src, dst_ref=dst, send_sem=send, recv_sem=recv, device_id=device, device_id_type=MESH
        )

    whole = (up_all, down_all)
    shards = (up_ref, down_ref)

    def view(item):
        s, dz, dx, part = item
        b, _, first, count = STREAMS[s]
        zz = lax.rem(z - dz + 2 * NZ, NZ)
        xx = lax.rem(x - dx + 2 * NX, NX)
        row = place(zz, xx, c) * SHARD
        rows = SHARD
        if part is not None:
            rows = SHARD // 2
            row = row + part * rows
        return whole[b].at[pl.ds(pl.multiple_of(row, 16), rows), pl.ds(first, count)]

    def own_view(s, part):
        b, _, first, count = STREAMS[s]
        if part is None:
            return shards[b].at[:, pl.ds(first, count)]
        return shards[b].at[pl.ds(part * (SHARD // 2), SHARD // 2), pl.ds(first, count)]

    def pass_on(item):
        s, dz, dx, part = item
        b = STREAMS[s][0]
        own = dz == 0 and dx == 0
        for axis, way, there in onward(item):
            here = (s, dz, dx, there[3])
            src = own_view(s, there[3]) if own else view(here)
            remote(src, view(here), send_sems.at[b], arrive.at[SLOT[there]], near(axis, way)).start()
        src = own_view(s, part) if own else view(item)
        remote(src, view(item), twin_sem.at[b], twin_arrive.at[b, DZ_ORDER.index(dz)], twin).start()

    def take(item):
        ref = view(item)
        remote(ref, ref, send_sems.at[0], arrive.at[SLOT[item]], twin).wait_recv()
        pass_on(item)

    queue = list(PLAN)

    def serve(until):
        while queue and queue[0][0] <= until:
            take(queue.pop(0)[1])

    def serve_for(b, dz):
        def missing():
            return any(STREAMS[i[0]][0] == b and i[1] == dz for _, i in queue)
        while missing():
            take(queue.pop(0)[1])

    def twin_wait(b, dz):
        ref = whole[b].at[pl.ds(0, NX * SHARD), :]
        remote(ref, ref, twin_sem.at[b], twin_arrive.at[b, DZ_ORDER.index(dz)], twin).wait_recv()

    for s in range(len(STREAMS)):
        pass_on((s, 0, 0, None))

    last = pl.ds(TOK - REACH, REACH)
    halo = [
        remote(k_ref.at[:, last], k_prev, halo_send.at[0], halo_sem.at[0], line(1)),
        remote(v_ref.at[:, last], v_prev, halo_send.at[1], halo_sem.at[1], line(1)),
        remote(docs_ref.at[:, last], docs_prev, halo_send.at[2], halo_sem.at[2], line(1)),
    ]
    for copy in halo:
        copy.start()

    own_row = pl.multiple_of(place(z, x, c) * SHARD, SHARD)
    up_all[pl.ds(own_row, SHARD), :] = up_ref[...]
    down_all[pl.ds(own_row, SHARD), :] = down_ref[...]

    k_band[:, REACH:] = k_ref[...]
    v_band[:, REACH:] = v_ref[...]
    docs_band[:, REACH:] = docs_ref[...].astype(jnp.float32)
    ahead = (
        REACH
        + lax.broadcasted_iota(jnp.int32, (REACH, 2 * REACH), 0)
        - lax.broadcasted_iota(jnp.int32, (REACH, 2 * REACH), 1)
    )
    in_reach = (ahead >= 0) & (ahead < REACH)

    def attend(block):
        rows = pl.ds(block * REACH, REACH)
        band = pl.ds(block * REACH, 2 * REACH)
        keys = k_band[:, band]
        values = v_band[:, band]
        own_docs = docs_band[:, pl.ds((block + 1) * REACH, REACH)]
        own_docs = jnp.transpose(jnp.broadcast_to(own_docs, (REACH, REACH)))
        own_docs = jnp.concatenate([own_docs, own_docs], axis=1)
        visible = in_reach & (own_docs == docs_band[:, band])
        outs = []
        for h in range(4):
            scores = jnp.dot(
                q_ref[rows, pl.ds(h * HEAD, HEAD)], keys, preferred_element_type=jnp.float32
            ) * HEAD ** (-0.5)
            scores = jnp.where(visible, scores, masked_score)
            sink = sink_ref[h]
            top = jnp.maximum(jnp.max(scores, axis=-1, keepdims=True), sink)
            exponent = jnp.where(visible, jnp.exp(scores - top), 0.0)
            total = jnp.exp(sink - top) + jnp.sum(exponent, axis=-1, keepdims=True)
            shares = (exponent / total).astype(jnp.bfloat16)
            outs.append(
                lax.dot_general(
                    shares, values, (((1,), (1,)), ((), ())), preferred_element_type=jnp.float32
                )
            )
        attended[rows, :] = jnp.concatenate(outs, axis=1).astype(jnp.bfloat16)

    attend(1)
    attend(2)
    serve(4.6)
    attend(3)
    attend(4)
    serve(5.6)
    for copy in halo:
        copy.wait_recv()
    k_band[:, :REACH] = k_prev[...]
    v_band[:, :REACH] = v_prev[...]
    docs_band[:, :REACH] = jnp.where(sp == 0, -1.0, docs_prev[...].astype(jnp.float32))
    attend(0)

    def owner_rows(of, part=None):
        if part is None:
            return pl.ds(pl.multiple_of(of * OWN, 16), OWN)
        return pl.ds(pl.multiple_of(of * OWN + part * HALF, 16), HALF)

    def lanes(of):
        return pl.ds(pl.multiple_of(of * 256, 256), 256)

    swaps = []
    for by in (1, 3, 2):
        swaps.append(remote(
            attended.at[owner_rows(lax.rem(y + by, NY)), :], heads.at[:, lanes(y)],
            swap_send.at[by - 1], swap_sem.at[by - 1], column(by),
        ))
        swaps[-1].start()
    heads[:, lanes(y)] = attended[owner_rows(y), :]
    serve(9.0)
    w_load.wait()
    res_load.wait()
    for by, copy in zip((1, 3, 2), swaps):
        slot = heads.at[:, lanes(lax.rem(y - by + NY, NY))]
        remote(slot, slot, swap_send.at[by - 1], swap_sem.at[by - 1], column(by)).wait_recv()

    def project(n, carry):
        cols = pl.ds(pl.multiple_of(n * 512, 512), 512)
        product = jnp.dot(heads[...], w_ref[:, cols], preferred_element_type=jnp.float32)
        product = product.astype(jnp.bfloat16).astype(jnp.float32)
        mixed[:, cols] = (res_ref[:, cols].astype(jnp.float32) + product).astype(jnp.bfloat16)
        return carry

    lax.fori_loop(0, 4, project, 0)

    def norm(i, carry):
        widened = mixed[pl.ds(pl.multiple_of(i * 32, 32), 32), :].astype(jnp.float32)
        scale = lax.rsqrt(jnp.mean(widened * widened, axis=-1, keepdims=True) + epsilon)
        normed[pl.ds(pl.multiple_of(y * OWN + i * 32, 32), 32), :] = (
            widened * scale * gain_ref[...]
        ).astype(jnp.bfloat16)
        return carry

    lax.fori_loop(0, 5, norm, 0)

    def row_copy(of, part, by, slot):
        ref = normed.at[owner_rows(of, part), :]
        return remote(ref, ref, row_send.at[0], row_sem.at[slot], column(by))

    row_copy(y, 0, 1, 0).start()
    row_copy(y, 1, -1, 3).start()
    row_copy(y, 1, 1, 1).start()
    row_copy(y, 0, -1, 2).start()
    before, after, across = lax.rem(y + 3, NY), lax.rem(y + 1, NY), lax.rem(y + 2, NY)
    serve(21.0)
    row_copy(before, 0, 1, 0).wait_recv()
    row_copy(before, 0, 1, 4).start()
    row_copy(after, 1, -1, 3).wait_recv()
    row_copy(after, 1, -1, 5).start()
    serve(29.0)
    row_copy(before, 1, 1, 1).wait_recv()
    row_copy(after, 0, -1, 2).wait_recv()
    serve(35.0)
    row_copy(across, 0, 1, 4).wait_recv()
    row_copy(across, 1, -1, 5).wait_recv()
    for dz in DZ_ORDER:
        serve_for(0, dz)
    for dz in DZ_ORDER:
        twin_wait(0, dz)

    def expand(n, carry):
        cols = pl.ds(pl.multiple_of(n * 512, 512), 512)
        before_act = jnp.dot(normed[...], up_all[:, cols], preferred_element_type=jnp.float32)
        hidden[:, cols] = jnp.square(jnp.maximum(before_act, 0.0)).astype(jnp.bfloat16)
        return carry

    for half in range(2):
        lax.fori_loop(2 * half, 2 * half + 2, expand, 0)
        serve(44.0)

    def add_and_send(i):
        for way, (first, last_buf, part) in enumerate(((first_a, last_a, 0), (first_b, last_b, 1))):
            by = 1 if way == 0 else -1
            to = lax.rem(y + by + NY, NY)
            ref = first.at[i]
            remote(ref, ref, sum_send.at[0], sum_sem.at[i, way], column(by)).wait_recv()
            rows = owner_rows(to, part)
            parts[i, rows, :] = (
                parts[i, rows, :].astype(jnp.float32) + first[i].astype(jnp.float32)
            ).astype(jnp.bfloat16)
            remote(parts.at[i, owner_rows(to), :], last_buf.at[i], sum_send.at[0], end_sem.at[i, way],
                   column(by)).start()

    for i, dz in enumerate(DZ_ORDER):
        serve_for(1, dz)
        twin_wait(1, dz)
        zz = lax.rem(z - dz + 2 * NZ, NZ)
        parts[i] = lax.dot_general(
            hidden[...], down_all[pl.ds(pl.multiple_of(zz * 256, 256), 256), :],
            (((1,), (1,)), ((), ())), preferred_element_type=jnp.float32,
        ).astype(jnp.bfloat16)
        remote(parts.at[i, owner_rows(across, 0), :], first_a.at[i], sum_send.at[0], sum_sem.at[i, 0],
               column(1)).start()
        remote(parts.at[i, owner_rows(across, 1), :], first_b.at[i], sum_send.at[0], sum_sem.at[i, 1],
               column(-1)).start()
        if i >= 1:
            add_and_send(i - 1)
    add_and_send(len(DZ_ORDER) - 1)
    for i, dz in enumerate(DZ_ORDER):
        zz = lax.rem(z - dz + 2 * NZ, NZ)
        for way, last_buf in enumerate((last_a, last_b)):
            ref = last_buf.at[i]
            remote(ref, ref, sum_send.at[0], end_sem.at[i, way], column(1)).wait_recv()
        branch = (
            parts[i, owner_rows(y), :].astype(jnp.float32)
            + last_a[i].astype(jnp.float32)
            + last_b[i].astype(jnp.float32)
        )
        branch = branch.astype(jnp.bfloat16).astype(jnp.float32)
        out_ref[:, lanes(zz)] = (mixed[:, lanes(zz)].astype(jnp.float32) + branch).astype(jnp.bfloat16)

    for b in range(2):
        ref = whole[b].at[pl.ds(0, 31 * SHARD), :]
        remote(ref, ref, send_sems.at[b], arrive.at[0], twin).wait_send()
        ref = whole[b].at[pl.ds(0, 32 * SHARD), :]
        remote(ref, ref, twin_sem.at[b], arrive.at[0], twin).wait_send()
    for copy in halo:
        copy.wait_send()
    for copy in swaps:
        copy.wait_send()
    ref = normed.at[pl.ds(0, 3 * OWN), :]
    remote(ref, ref, row_send.at[0], arrive.at[0], twin).wait_send()
    ref = parts.at[:, pl.ds(0, 3 * OWN), :]
    remote(ref, ref, sum_send.at[0], arrive.at[0], twin).wait_send()


def body(
    queries, keys, values, documents, sinks, out_weight, residual, norm_gain, up_weight, down_weight
):
    vmem = pl.BlockSpec(memory_space=pltpu.VMEM)
    anywhere = pl.BlockSpec(memory_space=pl.ANY)
    bf16 = jnp.bfloat16
    dma = pltpu.SemaphoreType.DMA
    blocks = len(DZ_ORDER)
    return pl.pallas_call(
        kernel,
        out_shape=jax.ShapeDtypeStruct((OWN, D), bf16),
        in_specs=[vmem, vmem, vmem, vmem, pl.BlockSpec(memory_space=pltpu.SMEM), anywhere, anywhere,
                  vmem, vmem, vmem],
        out_specs=vmem,
        scratch_shapes=[
            pltpu.VMEM((D, D), bf16),
            pltpu.VMEM((D, D), bf16),
            pltpu.VMEM((1024, D), bf16),
            pltpu.VMEM((OWN, D), bf16),
            pltpu.VMEM((HEAD, TOK + REACH), bf16),
            pltpu.VMEM((HEAD, TOK + REACH), bf16),
            pltpu.VMEM((HEAD, REACH), bf16),
            pltpu.VMEM((HEAD, REACH), bf16),
            pltpu.VMEM((1, REACH), jnp.int32),
            pltpu.VMEM((1, TOK + REACH), jnp.float32),
            pltpu.VMEM((TOK, 256), bf16),
            pltpu.VMEM((OWN, 1024), bf16),
            pltpu.VMEM((OWN, D), bf16),
            pltpu.VMEM((TOK, D), bf16),
            pltpu.VMEM((TOK, D), bf16),
            pltpu.VMEM((blocks, TOK, 256), bf16),
            pltpu.VMEM((blocks, HALF, 256), bf16),
            pltpu.VMEM((blocks, HALF, 256), bf16),
            pltpu.VMEM((blocks, OWN, 256), bf16),
            pltpu.VMEM((blocks, OWN, 256), bf16),
            dma((len(PLAN),)),
            dma((2,)),
            dma((2,)),
            dma((2, blocks)),
            dma((2,)),
            dma((3,)),
            dma((3,)),
            dma((3,)),
            dma((3,)),
            dma((6,)),
            dma((1,)),
            dma((blocks, 2)),
            dma((1,)),
            dma((blocks, 2)),
        ],
        compiler_params=pltpu.CompilerParams(
            collective_id=0, has_side_effects=True, vmem_limit_bytes=60 * 1024 * 1024
        ),
    )(
        queries, keys.T, values.T, documents.reshape(1, TOK), sinks, out_weight, residual,
        norm_gain.reshape(1, D), up_weight, down_weight.T,
    )


def solution(mesh):
    in_specs = (
        P("sp", "tp"),
        P("sp", "tp"),
        P("sp", "tp"),
        P("sp"),
        P("tp"),
        P(),
        P(("sp", "tp"), None),
        P(),
        P("sp", "tp"),
        P("tp", "sp"),
    )
    out_specs = P(("sp", "tp"), None)
    return jax.shard_map(body, mesh=mesh, in_specs=in_specs, out_specs=out_specs, check_vma=False)
```

```python
import functools
import heapq

import jax
import jax.numpy as jnp
from jax import lax
from jax.experimental import pallas as pl
from jax.experimental.pallas import tpu as pltpu
from jax.sharding import PartitionSpec as P

MESH = pl.DeviceIdType.MESH
NZ, NX, NY = 8, 4, 4
HEAD = 64
REACH = 128
TOK = 640
OWN = 160
HALF = 80
D = 2048
SHARD = 32
masked_score = -1e30
epsilon = 1e-06

CUT = 1280
STREAMS = ((0, "z", 0, CUT), (0, "x", CUT, D - CUT), (1, "z", 0, CUT), (1, "x", CUT, D - CUT))
BEGIN = (0.0, 0.0, 20.0, 20.0)
RATE = 46.6e3
LATENCY = 1.8
TWIN_RATE = 600e3
TWIN_LATENCY = 1.0
ISSUE = 0.015
MARGIN = 0.3
LAG = 3
DZ_ORDER = (0, 1, -1, 2, -2, 3, -3, 4)


def onward(item):
    s, dz, dx, part = item
    mode = STREAMS[s][1]
    out = []

    def along_z():
        if dz == 0:
            out.append(("z", 1, (s, 1, dx, None)))
            out.append(("z", -1, (s, -1, dx, None)))
        elif dz in (1, 2):
            out.append(("z", 1, (s, dz + 1, dx, None)))
        elif dz in (-1, -2):
            out.append(("z", -1, (s, dz - 1, dx, None)))
        elif dz == 3:
            out.append(("z", 1, (s, 4, dx, 0)))
        elif dz == -3:
            out.append(("z", -1, (s, 4, dx, 1)))

    def along_x():
        if dx == 0:
            out.append(("x", 1, (s, dz, 1, part)))
            out.append(("x", -1, (s, dz, -1, part)))
        elif dx == 1:
            if dz == 0:
                out.append(("x", 1, (s, dz, 2, 0)))
            elif dz in (1, -2, 3) or (dz == 4 and part == 0):
                out.append(("x", 1, (s, dz, 2, part)))
        elif dx == -1:
            if dz == 0:
                out.append(("x", -1, (s, dz, 2, 1)))
            elif dz in (-1, 2, -3) or (dz == 4 and part == 1):
                out.append(("x", -1, (s, dz, 2, part)))

    if mode == "z":
        if dx == 0:
            along_z()
        along_x()
    else:
        if dz == 0:
            along_x()
        if part is None or dz != 0:
            if part is None:
                along_z()
        elif part == 1:
            along_z()
    return out


def size(item):
    return SHARD * STREAMS[item[0]][3] * 2 // (1 if item[3] is None else 2)


def arrivals():
    found, items = [(s, 0, 0, None) for s in range(len(STREAMS))], []
    while found:
        for _, _, there in onward(found.pop()):
            items.append(there)
            found.append(there)
    return sorted(items, key=str)


SLOT = {item: k for k, item in enumerate(arrivals())}


class Clock:
    def __init__(self):
        self.now = 0.0
        self.free = {}
        self.due = {}
        self.coming = []
        for s, begin in enumerate(BEGIN):
            item = (s, 0, 0, None)
            heapq.heappush(self.coming, (begin, str(item), item))

    def send(self, link, count, label, rate=RATE, latency=LATENCY):
        self.now += ISSUE
        end = max(self.now, self.free.get(link, 0.0)) + count / rate
        self.free[link] = end
        self.due[label] = max(self.due.get(label, 0.0), end + latency)

    def expect(self, item):
        heapq.heappush(self.coming, (self.due[item] + MARGIN, str(item), item))


PIECES = {
    0: ((0, 0, 128),),
    1: ((0, 128, 32), (1, 0, 96)),
    2: ((1, 96, 64), (2, 0, 64)),
    3: ((2, 64, 96), (3, 0, 32)),
    4: ((3, 32, 128),),
}
ITEMS = ((0, 0),) + tuple((h, i) for i in range(8) for h in range(2) if (h, i) != (0, 0))


def kernel(
    q_hbm, k_hbm, v_hbm, docs_hbm, sink_ref, w_hbm, res_hbm, gain_hbm, up_hbm, down_hbm,
    out_hbm,
    up_all, down_all, w_ref, res_ref, q_ref, k_ref, v_ref, docs_ref, gain_ref, up_ref, down_ref,
    k_band, v_band, k_prev, v_prev, docs_prev, docs_band,
    attended, heads, mixed, normed, hidden, parts, first_a, first_b, last_a, last_b, out_ref,
    arrive, send_sems, twin_sem, twin_arrive, load_sem, halo_sem, halo_send,
    swap_sem, swap_send, row_sem, row_send, sum_sem, sum_send, end_sem, out_sem,
):
    sp = lax.axis_index("sp")
    y = lax.axis_index("tp")
    c = lax.rem(sp, 2)
    x = lax.rem(sp // 2, NX)
    z = sp // (2 * NX)

    def place(zz, xx, cc):
        return (zz * NX + xx) * 2 + cc

    def near(axis, way):
        if axis == "z":
            return {"sp": place(lax.rem(z + way + NZ, NZ), x, c), "tp": y}
        return {"sp": place(z, lax.rem(x + way + NX, NX), c), "tp": y}

    twin = {"sp": place(z, x, 1 - c), "tp": y}

    def column(by):
        return {"sp": sp, "tp": lax.rem(y + by + NY, NY)}

    def line(by):
        return {"sp": lax.rem(sp + by + 2 * NX * NZ, 2 * NX * NZ), "tp": y}

    up_load, down_load, k_load, v_load, docs_load, q_load, gain_load, res_load, w_load = loads = [
        pltpu.make_async_copy(src, dst, load_sem.at[n])
        for n, (src, dst) in enumerate((
            (up_hbm, up_ref), (down_hbm, down_ref), (k_hbm, k_ref), (v_hbm, v_ref), (docs_hbm, docs_ref),
            (q_hbm, q_ref), (gain_hbm, gain_ref), (res_hbm, res_ref), (w_hbm, w_ref),
        ))
    ]
    for load in loads:
        load.start()

    barrier = pltpu.get_barrier_semaphore()
    greeted = [near("z", 1), near("z", -1), near("x", 1), near("x", -1), twin,
               column(1), column(2), column(3), line(1), line(-1)]
    for device in greeted:
        pl.semaphore_signal(barrier, inc=1, device_id=device, device_id_type=MESH)
    pl.semaphore_wait(barrier, len(greeted))

    def remote(src, dst, send, recv, device):
        return pltpu.make_async_remote_copy(
            src_ref=src, dst_ref=dst, send_sem=send, recv_sem=recv, device_id=device, device_id_type=MESH
        )

    whole = (up_all, down_all)
    shards = (up_ref, down_ref)

    def view(item):
        s, dz, dx, part = item
        b, _, first, count = STREAMS[s]
        zz = lax.rem(z - dz + 2 * NZ, NZ)
        xx = lax.rem(x - dx + 2 * NX, NX)
        row = place(zz, xx, c) * SHARD
        rows = SHARD
        if part is not None:
            rows = SHARD // 2
            row = row + part * rows
        return whole[b].at[pl.ds(pl.multiple_of(row, 16), rows), pl.ds(first, count)]

    def own_view(s, part):
        b, _, first, count = STREAMS[s]
        if part is None:
            return shards[b].at[:, pl.ds(first, count)]
        return shards[b].at[pl.ds(part * (SHARD // 2), SHARD // 2), pl.ds(first, count)]

    clock = Clock()
    halves = set()
    left = {(b, dz): NX * SHARD * D * 2 for b in range(2) for dz in DZ_ORDER}

    def pass_on(item):
        s, dz, dx, part = item
        b = STREAMS[s][0]
        own = dz == 0 and dx == 0
        sent = onward(item)
        if STREAMS[s][1] == "x" and dz == 0 and dx == 2:
            halves.add(item)
            sent = onward((s, 0, 2, 1)) if {(s, 0, 2, 0), (s, 0, 2, 1)} <= halves else []
        for axis, way, there in sent:
            here = (s, dz, dx, there[3])
            src = own_view(s, there[3]) if own else view(here)
            remote(src, view(here), send_sems.at[b], arrive.at[SLOT[there]], near(axis, way)).start()
            clock.send((axis, way), size(there), there)
            clock.expect(there)
        src = own_view(s, part) if own else view(item)
        remote(src, view(item), twin_sem.at[b], twin_arrive.at[b, DZ_ORDER.index(dz)], twin).start()
        clock.send("twin", size(item), ("twin", b, dz), TWIN_RATE, TWIN_LATENCY)
        left[b, dz] -= size(item)

    def take():
        moment, _, item = heapq.heappop(clock.coming)
        clock.now = max(clock.now, moment)
        if item[1] != 0 or item[2] != 0:
            ref = view(item)
            remote(ref, ref, send_sems.at[0], arrive.at[SLOT[item]], twin).wait_recv()
        pass_on(item)

    def work(us):
        clock.now += us
        while clock.coming and clock.coming[0][0] <= clock.now:
            take()

    def hold(label):
        while clock.coming and clock.coming[0][0] < clock.due[label]:
            take()
        clock.now = max(clock.now, clock.due[label])

    def weights(b, dz):
        while left[b, dz] > 0:
            take()
        hold(("twin", b, dz))
        ref = whole[b].at[pl.ds(0, NX * SHARD), :]
        remote(ref, ref, twin_sem.at[b], twin_arrive.at[b, DZ_ORDER.index(dz)], twin).wait_recv()

    up_load.wait()
    work(0.0)
    for load in (k_load, v_load, docs_load):
        load.wait()

    last = pl.ds(TOK - REACH, REACH)
    docs_band[:, REACH:] = docs_ref[...].reshape(1, TOK).astype(jnp.float32)
    halo = [
        remote(k_ref.at[:, last], k_prev, halo_send.at[0], halo_sem.at[0], line(1)),
        remote(v_ref.at[:, last], v_prev, halo_send.at[1], halo_sem.at[1], line(1)),
        remote(docs_ref.at[last], docs_prev, halo_send.at[2], halo_sem.at[2], line(1)),
    ]
    for copy in halo:
        copy.start()
    clock.send("halo", 2 * HEAD * REACH * 2, "halo", RATE, 2 * LATENCY)

    own_row = pl.multiple_of(place(z, x, c) * SHARD, SHARD)
    up_all[pl.ds(own_row, SHARD), :] = up_ref[...]

    k_band[:, REACH:] = k_ref[...]
    v_band[:, REACH:] = v_ref[...]
    down_load.wait()
    down_all[pl.ds(own_row, SHARD), :] = down_ref[...]
    q_load.wait()
    ahead = (
        REACH
        + lax.broadcasted_iota(jnp.int32, (REACH, 2 * REACH), 0)
        - lax.broadcasted_iota(jnp.int32, (REACH, 2 * REACH), 1)
    )
    in_reach = (ahead >= 0) & (ahead < REACH)

    def attend(block):
        rows = pl.ds(block * REACH, REACH)
        band = pl.ds(block * REACH, 2 * REACH)
        keys = k_band[:, band]
        values = v_band[:, band]
        own_docs = docs_band[:, pl.ds((block + 1) * REACH, REACH)]
        own_docs = jnp.transpose(jnp.broadcast_to(own_docs, (REACH, REACH)))
        own_docs = jnp.concatenate([own_docs, own_docs], axis=1)
        visible = in_reach & (own_docs == docs_band[:, band])
        outs = []
        for h in range(4):
            scores = jnp.dot(
                q_ref[rows, pl.ds(h * HEAD, HEAD)], keys, preferred_element_type=jnp.float32
            ) * HEAD ** (-0.5)
            scores = jnp.where(visible, scores, masked_score)
            sink = sink_ref[h]
            top = jnp.maximum(jnp.max(scores, axis=-1, keepdims=True), sink)
            exponent = jnp.where(visible, jnp.exp(scores - top), 0.0)
            total = jnp.exp(sink - top) + jnp.sum(exponent, axis=-1, keepdims=True)
            shares = (exponent / total).astype(jnp.bfloat16)
            outs.append(
                lax.dot_general(
                    shares, values, (((1,), (1,)), ((), ())), preferred_element_type=jnp.float32
                )
            )
        attended[rows, :] = jnp.concatenate(outs, axis=1).astype(jnp.bfloat16)

    def lanes(of):
        return pl.ds(pl.multiple_of(of * 256, 256), 256)

    def hand_over(block):
        for owner, first, rows in PIECES[block]:
            @pl.when(y != owner)
            def _():
                remote(
                    attended.at[pl.ds(owner * OWN + first, rows), :], heads.at[pl.ds(first, rows), lanes(y)],
                    swap_send.at[0], swap_sem.at[y], {"sp": sp, "tp": owner},
                ).start()

    for block in (1, 2, 3):
        attend(block)
        hand_over(block)
        work(0.88)
    hold("halo")
    for copy in halo:
        copy.wait_recv()
    k_band[:, :REACH] = k_prev[...]
    v_band[:, :REACH] = v_prev[...]
    docs_band[:, :REACH] = jnp.where(sp == 0, -1.0, docs_prev[...].reshape(1, REACH).astype(jnp.float32))
    attend(0)
    hand_over(0)
    work(0.88)
    attend(4)
    hand_over(4)
    for by in (1, 3, 2):
        clock.send(("y", 1 if by < 3 else -1), OWN * 256 * 2, ("swap", by))
    heads[:, lanes(y)] = attended[pl.ds(pl.multiple_of(y * OWN, 32), OWN), :]
    work(0.1)
    w_load.wait()
    res_load.wait()
    gain_load.wait()
    for by in (1, 3, 2):
        other = lax.rem(y + by, NY)
        slot = heads.at[:, lanes(other)]
        hold(("swap", by))
        remote(slot, slot, swap_send.at[0], swap_sem.at[other], column(by)).wait_recv()

    def project(n, carry):
        cols = pl.ds(pl.multiple_of(n * 512, 512), 512)
        product = jnp.dot(heads[...], w_ref[:, cols], preferred_element_type=jnp.float32)
        product = product.astype(jnp.bfloat16).astype(jnp.float32)
        mixed[:, cols] = (res_ref[:, cols].astype(jnp.float32) + product).astype(jnp.bfloat16)
        return carry

    for half in range(2):
        lax.fori_loop(2 * half, 2 * half + 2, project, 0)
        work(0.75)

    def norm(h):
        def step(i, carry):
            rows = pl.ds(pl.multiple_of(h * HALF + i * 16, 16), 16)
            widened = mixed[rows, :].astype(jnp.float32)
            scale = lax.rsqrt(jnp.mean(widened * widened, axis=-1, keepdims=True) + epsilon)
            normed[pl.ds(pl.multiple_of((h * NY + y) * HALF + i * 16, 16), 16), :] = (
                widened * scale * gain_ref[...]
            ).astype(jnp.bfloat16)
            return carry

        lax.fori_loop(0, 5, step, 0)

    before, after, across = lax.rem(y + 3, NY), lax.rem(y + 1, NY), lax.rem(y + 2, NY)

    def row_copy(h, of, side, by, slot):
        ref = normed.at[pl.ds(pl.multiple_of((h * NY + of) * HALF, 16), HALF), pl.ds(side * (D // 2), D // 2)]
        return remote(ref, ref, row_send.at[0], row_sem.at[h, slot], column(by))

    def rows_sent(h, of, side, by, slot):
        row_copy(h, of, side, by, slot).start()
        clock.send(("y", by), HALF * D, ("row", h, slot))

    def rows_come(h, of, side, by, slot):
        hold(("row", h, slot))
        row_copy(h, of, side, by, slot).wait_recv()

    def rows_out(h):
        rows_sent(h, y, 0, 1, 0)
        rows_sent(h, y, 1, -1, 3)
        rows_sent(h, y, 1, 1, 1)
        rows_sent(h, y, 0, -1, 2)

    def rows_on(h):
        rows_come(h, before, 0, 1, 0)
        rows_sent(h, before, 0, 1, 4)
        rows_come(h, after, 1, -1, 3)
        rows_sent(h, after, 1, -1, 5)

    def rows_in(h):
        rows_come(h, before, 1, 1, 1)
        rows_come(h, after, 0, -1, 2)
        rows_come(h, across, 0, 1, 4)
        rows_come(h, across, 1, -1, 5)

    norm(0)
    rows_out(0)
    norm(1)
    work(0.4)
    rows_on(0)
    rows_out(1)
    rows_in(0)
    rows_on(1)
    for dz in DZ_ORDER:
        weights(0, dz)

    def expand(h, begin, end):
        rows = pl.ds(h * NY * HALF, NY * HALF)

        def step(n):
            cols = pl.ds(n * 512, 512)
            before_act = jnp.dot(normed[rows, :], up_all[:, cols], preferred_element_type=jnp.float32)
            hidden[rows, cols] = jnp.square(jnp.maximum(before_act, 0.0)).astype(jnp.bfloat16)

        for n in range(begin, end):
            step(n)
            work(0.8)

    def owner_rows(of):
        return pl.ds(pl.multiple_of(of * HALF, 16), HALF)

    side_a, side_b = pl.ds(0, 128), pl.ds(128, 128)
    there = set()

    def contract(h, i):
        dz = DZ_ORDER[i]
        k = h * 8 + i
        if dz not in there:
            weights(1, dz)
            there.add(dz)
        zz = lax.rem(z - dz + 2 * NZ, NZ)
        parts[k] = lax.dot_general(
            hidden[pl.ds(h * NY * HALF, NY * HALF), :], down_all[pl.ds(pl.multiple_of(zz * 256, 256), 256), :],
            (((1,), (1,)), ((), ())), preferred_element_type=jnp.float32,
        ).astype(jnp.bfloat16)
        remote(parts.at[k, owner_rows(across), side_a], first_a.at[k], sum_send.at[0], sum_sem.at[k, 0],
               column(1)).start()
        remote(parts.at[k, owner_rows(across), side_b], first_b.at[k], sum_send.at[0], sum_sem.at[k, 1],
               column(-1)).start()
        work(0.45)
        clock.send(("y", 1), HALF * 256, ("sum", k, 0))
        clock.send(("y", -1), HALF * 256, ("sum", k, 1))

    def add_and_send(h, i):
        k = h * 8 + i
        for way, (first, final, side, to, by) in enumerate((
            (first_a, last_a, side_a, after, 1), (first_b, last_b, side_b, before, -1),
        )):
            ref = first.at[k]
            hold(("sum", k, way))
            remote(ref, ref, sum_send.at[0], sum_sem.at[k, way], column(by)).wait_recv()
            rows = owner_rows(to)
            parts[k, rows, side] = (
                parts[k, rows, side].astype(jnp.float32) + first[k].astype(jnp.float32)
            ).astype(jnp.bfloat16)
            remote(parts.at[k, rows, :], final.at[k], sum_send.at[0], end_sem.at[k, way], column(by)).start()
            clock.now += 0.03
            clock.send(("y", by), HALF * 512, ("end", k, way))

    def finish(h, i):
        k = h * 8 + i
        zz = lax.rem(z - DZ_ORDER[i] + 2 * NZ, NZ)
        for way, final in enumerate((last_a, last_b)):
            ref = final.at[k]
            hold(("end", k, way))
            remote(ref, ref, sum_send.at[0], end_sem.at[k, way], column(1)).wait_recv()
        branch = (
            parts[k, owner_rows(y), :].astype(jnp.float32)
            + last_a[k].astype(jnp.float32)
            + last_b[k].astype(jnp.float32)
        )
        branch = branch.astype(jnp.bfloat16).astype(jnp.float32)
        rows = pl.ds(h * HALF, HALF)
        out_ref[rows, lanes(zz)] = (mixed[rows, lanes(zz)].astype(jnp.float32) + branch).astype(jnp.bfloat16)
        pltpu.make_async_copy(out_ref.at[rows, lanes(zz)], out_hbm.at[rows, lanes(zz)], out_sem.at[0]).start()

    expand(0, 0, 4)
    contract(*ITEMS[0])
    rows_in(1)
    expand(1, 0, 4)
    for n in range(1, len(ITEMS)):
        contract(*ITEMS[n])
        if n >= LAG:
            add_and_send(*ITEMS[n - LAG])
    for n in range(len(ITEMS) - LAG, len(ITEMS)):
        add_and_send(*ITEMS[n])
    for item in ITEMS:
        finish(*item)
    assert not clock.coming

    for b in range(2):
        ref = whole[b].at[pl.ds(0, 31 * SHARD), :]
        remote(ref, ref, send_sems.at[b], arrive.at[0], twin).wait_send()
        ref = whole[b].at[pl.ds(0, 32 * SHARD), :]
        remote(ref, ref, twin_sem.at[b], arrive.at[0], twin).wait_send()
    for copy in halo:
        copy.wait_send()
    ref = attended.at[pl.ds(0, 3 * OWN), :]
    remote(ref, ref, swap_send.at[0], arrive.at[0], twin).wait_send()
    ref = normed.at[pl.ds(0, 3 * OWN), :]
    remote(ref, ref, row_send.at[0], arrive.at[0], twin).wait_send()
    ref = parts.at[:, pl.ds(0, 3 * HALF), :]
    remote(ref, ref, sum_send.at[0], arrive.at[0], twin).wait_send()
    pltpu.make_async_copy(out_ref, out_hbm, out_sem.at[0]).wait()


def body(
    queries, keys, values, documents, sinks, out_weight, residual, norm_gain, up_weight, down_weight
):
    anywhere = pl.BlockSpec(memory_space=pl.ANY)
    bf16 = jnp.bfloat16
    dma = pltpu.SemaphoreType.DMA
    blocks = len(DZ_ORDER)
    return pl.pallas_call(
        kernel,
        out_shape=jax.ShapeDtypeStruct((OWN, D), bf16),
        in_specs=[anywhere] * 4 + [pl.BlockSpec(memory_space=pltpu.SMEM)] + [anywhere] * 5,
        out_specs=anywhere,
        scratch_shapes=[
            pltpu.VMEM((D, D), bf16),
            pltpu.VMEM((D, D), bf16),
            pltpu.VMEM((1024, D), bf16),
            pltpu.VMEM((OWN, D), bf16),
            pltpu.VMEM((TOK, 256), bf16),
            pltpu.VMEM((HEAD, TOK), bf16),
            pltpu.VMEM((HEAD, TOK), bf16),
            pltpu.VMEM((TOK,), jnp.int32),
            pltpu.VMEM((1, D), jnp.float32),
            pltpu.VMEM((SHARD, D), bf16),
            pltpu.VMEM((SHARD, D), bf16),
            pltpu.VMEM((HEAD, TOK + REACH), bf16),
            pltpu.VMEM((HEAD, TOK + REACH), bf16),
            pltpu.VMEM((HEAD, REACH), bf16),
            pltpu.VMEM((HEAD, REACH), bf16),
            pltpu.VMEM((REACH,), jnp.int32),
            pltpu.VMEM((1, TOK + REACH), jnp.float32),
            pltpu.VMEM((TOK, 256), bf16),
            pltpu.VMEM((OWN, 1024), bf16),
            pltpu.VMEM((OWN, D), bf16),
            pltpu.VMEM((TOK, D), bf16),
            pltpu.VMEM((TOK, D), bf16),
            pltpu.VMEM((2 * blocks, NY * HALF, 256), bf16),
            pltpu.VMEM((2 * blocks, HALF, 128), bf16),
            pltpu.VMEM((2 * blocks, HALF, 128), bf16),
            pltpu.VMEM((2 * blocks, HALF, 256), bf16),
            pltpu.VMEM((2 * blocks, HALF, 256), bf16),
            pltpu.VMEM((OWN, D), bf16),
            dma((len(SLOT),)),
            dma((2,)),
            dma((2,)),
            dma((2, blocks)),
            dma((9,)),
            dma((3,)),
            dma((3,)),
            dma((NY,)),
            dma((1,)),
            dma((2, 6)),
            dma((1,)),
            dma((2 * blocks, 2)),
            dma((1,)),
            dma((2 * blocks, 2)),
            dma((1,)),
        ],
        compiler_params=pltpu.CompilerParams(
            collective_id=0, has_side_effects=True, vmem_limit_bytes=60 * 1024 * 1024
        ),
    )(
        queries, keys.T, values.T, documents, sinks, out_weight, residual,
        norm_gain.reshape(1, D), up_weight, down_weight.T,
    )


def solution(mesh):
    in_specs = (
        P("sp", "tp"),
        P("sp", "tp"),
        P("sp", "tp"),
        P("sp"),
        P("tp"),
        P(),
        P(("sp", "tp"), None),
        P(),
        P("sp", "tp"),
        P("tp", "sp"),
    )
    out_specs = P(("sp", "tp"), None)
    return jax.shard_map(body, mesh=mesh, in_specs=in_specs, out_specs=out_specs, check_vma=False)
```

```python
import functools
import heapq

import jax
import jax.numpy as jnp
from jax import lax
from jax.experimental import pallas as pl
from jax.experimental.pallas import tpu as pltpu
from jax.sharding import PartitionSpec as P

MESH = pl.DeviceIdType.MESH
NZ, NX, NY = 8, 4, 4
HEAD = 64
REACH = 128
TOK = 640
OWN = 160
HALF = 80
D = 2048
SHARD = 32
masked_score = -1e30
epsilon = 1e-06

CUT = 1280
STREAMS = ((0, "z", 0, CUT), (0, "x", CUT, D - CUT), (1, "z", 0, 1152), (1, "x", 1152, D - 1152))
BEGIN = (0.0, 0.0, 20.0, 17.0)
RATE = 46.6e3
LATENCY = 1.8
TWIN_RATE = 600e3
TWIN_LATENCY = 1.0
ISSUE = 0.015
MARGIN = 0.3
LAG = 3
DZ_ORDER = (0, 1, -1, 2, -2, 3, -3, 4)


def onward(item):
    s, dz, dx, part = item
    mode = STREAMS[s][1]
    out = []

    def along_z():
        if dz == 0:
            out.append(("z", 1, (s, 1, dx, None)))
            out.append(("z", -1, (s, -1, dx, None)))
        elif dz in (1, 2):
            out.append(("z", 1, (s, dz + 1, dx, None)))
        elif dz in (-1, -2):
            out.append(("z", -1, (s, dz - 1, dx, None)))
        elif dz == 3:
            out.append(("z", 1, (s, 4, dx, 0)))
        elif dz == -3:
            out.append(("z", -1, (s, 4, dx, 1)))

    def along_x():
        if dx == 0:
            out.append(("x", 1, (s, dz, 1, part)))
            out.append(("x", -1, (s, dz, -1, part)))
        elif dx == 1:
            if dz == 0:
                out.append(("x", 1, (s, dz, 2, 0)))
            elif dz in (1, -2, 3) or (dz == 4 and part == 0):
                out.append(("x", 1, (s, dz, 2, part)))
        elif dx == -1:
            if dz == 0:
                out.append(("x", -1, (s, dz, 2, 1)))
            elif dz in (-1, 2, -3) or (dz == 4 and part == 1):
                out.append(("x", -1, (s, dz, 2, part)))

    if mode == "z":
        if dx == 0:
            along_z()
        along_x()
    else:
        if dz == 0:
            along_x()
        if part is None or dz != 0:
            if part is None:
                along_z()
        elif part == 1:
            along_z()
    return out


def size(item):
    return SHARD * STREAMS[item[0]][3] * 2 // (1 if item[3] is None else 2)


def arrivals():
    found, items = [(s, 0, 0, None) for s in range(len(STREAMS))], []
    while found:
        for _, _, there in onward(found.pop()):
            items.append(there)
            found.append(there)
    return sorted(items, key=str)


SLOT = {item: k for k, item in enumerate(arrivals())}


class Clock:
    def __init__(self):
        self.now = 0.0
        self.free = {}
        self.due = {}
        self.coming = []
        for s, begin in enumerate(BEGIN):
            item = (s, 0, 0, None)
            heapq.heappush(self.coming, (begin, str(item), item))

    def send(self, link, count, label, rate=RATE, latency=LATENCY):
        self.now += ISSUE
        end = max(self.now, self.free.get(link, 0.0)) + count / rate
        self.free[link] = end
        self.due[label] = max(self.due.get(label, 0.0), end + latency)

    def expect(self, item):
        heapq.heappush(self.coming, (self.due[item] + MARGIN, str(item), item))


PIECES = {
    0: ((0, 0, 128),),
    1: ((0, 128, 32), (1, 0, 96)),
    2: ((1, 96, 64), (2, 0, 64)),
    3: ((2, 64, 96), (3, 0, 32)),
    4: ((3, 32, 128),),
}
ITEMS = ((0, 0),) + tuple((h, i) for i in range(8) for h in range(2) if (h, i) != (0, 0))


def kernel(
    q_hbm, k_hbm, v_hbm, docs_hbm, sink_ref, w_hbm, res_hbm, gain_hbm, up_hbm, down_hbm,
    out_hbm,
    up_all, down_all, w_ref, res_ref, q_ref, k_ref, v_ref, docs_ref, gain_ref, up_ref, down_ref,
    k_band, v_band, k_prev, v_prev, docs_prev, docs_band,
    attended, heads, mixed, normed, hidden, parts, first_a, first_b, last_a, last_b, out_ref,
    arrive, send_sems, twin_sem, twin_arrive, load_sem, halo_sem, halo_send,
    swap_sem, swap_send, row_sem, row_send, sum_sem, sum_send, end_sem, out_sem,
):
    sp = lax.axis_index("sp")
    y = lax.axis_index("tp")
    c = lax.rem(sp, 2)
    x = lax.rem(sp // 2, NX)
    z = sp // (2 * NX)

    def place(zz, xx, cc):
        return (zz * NX + xx) * 2 + cc

    def near(axis, way):
        if axis == "z":
            return {"sp": place(lax.rem(z + way + NZ, NZ), x, c), "tp": y}
        return {"sp": place(z, lax.rem(x + way + NX, NX), c), "tp": y}

    twin = {"sp": place(z, x, 1 - c), "tp": y}

    def column(by):
        return {"sp": sp, "tp": lax.rem(y + by + NY, NY)}

    def line(by):
        return {"sp": lax.rem(sp + by + 2 * NX * NZ, 2 * NX * NZ), "tp": y}

    up_load, down_load, k_load, v_load, docs_load, q_load, gain_load, res_load, w_load = loads = [
        pltpu.make_async_copy(src, dst, load_sem.at[n])
        for n, (src, dst) in enumerate((
            (up_hbm, up_ref), (down_hbm, down_ref), (k_hbm, k_ref), (v_hbm, v_ref), (docs_hbm, docs_ref),
            (q_hbm, q_ref), (gain_hbm, gain_ref), (res_hbm, res_ref), (w_hbm, w_ref),
        ))
    ]
    for load in loads:
        load.start()

    barrier = pltpu.get_barrier_semaphore()
    greeted = [near("z", 1), near("z", -1), near("x", 1), near("x", -1), twin,
               column(1), column(2), column(3), line(1), line(-1)]
    for device in greeted:
        pl.semaphore_signal(barrier, inc=1, device_id=device, device_id_type=MESH)
    pl.semaphore_wait(barrier, len(greeted))

    def remote(src, dst, send, recv, device):
        return pltpu.make_async_remote_copy(
            src_ref=src, dst_ref=dst, send_sem=send, recv_sem=recv, device_id=device, device_id_type=MESH
        )

    whole = (up_all, down_all)
    shards = (up_ref, down_ref)

    def view(item):
        s, dz, dx, part = item
        b, _, first, count = STREAMS[s]
        zz = lax.rem(z - dz + 2 * NZ, NZ)
        xx = lax.rem(x - dx + 2 * NX, NX)
        row = place(zz, xx, c) * SHARD
        rows = SHARD
        if part is not None:
            rows = SHARD // 2
            row = row + part * rows
        return whole[b].at[pl.ds(pl.multiple_of(row, 16), rows), pl.ds(first, count)]

    def own_view(s, part):
        b, _, first, count = STREAMS[s]
        if part is None:
            return shards[b].at[:, pl.ds(first, count)]
        return shards[b].at[pl.ds(part * (SHARD // 2), SHARD // 2), pl.ds(first, count)]

    clock = Clock()
    halves = set()
    left = {(b, dz): NX * SHARD * D * 2 for b in range(2) for dz in DZ_ORDER}

    def pass_on(item):
        s, dz, dx, part = item
        b = STREAMS[s][0]
        own = dz == 0 and dx == 0
        sent = onward(item)
        if STREAMS[s][1] == "x" and dz == 0 and dx == 2:
            halves.add(item)
            sent = onward((s, 0, 2, 1)) if {(s, 0, 2, 0), (s, 0, 2, 1)} <= halves else []
        for axis, way, there in sent:
            here = (s, dz, dx, there[3])
            src = own_view(s, there[3]) if own else view(here)
            remote(src, view(here), send_sems.at[b], arrive.at[SLOT[there]], near(axis, way)).start()
            clock.send((axis, way), size(there), there)
            clock.expect(there)
        src = own_view(s, part) if own else view(item)
        remote(src, view(item), twin_sem.at[b], twin_arrive.at[b, DZ_ORDER.index(dz)], twin).start()
        clock.send("twin", size(item), ("twin", b, dz), TWIN_RATE, TWIN_LATENCY)
        left[b, dz] -= size(item)

    def take():
        moment, _, item = heapq.heappop(clock.coming)
        clock.now = max(clock.now, moment)
        if item[1] != 0 or item[2] != 0:
            ref = view(item)
            remote(ref, ref, send_sems.at[0], arrive.at[SLOT[item]], twin).wait_recv()
        pass_on(item)

    def work(us):
        clock.now += us
        while clock.coming and clock.coming[0][0] <= clock.now:
            take()

    def hold(label):
        while clock.coming and clock.coming[0][0] < clock.due[label]:
            take()
        clock.now = max(clock.now, clock.due[label])

    def weights(b, dz):
        while left[b, dz] > 0:
            take()
        hold(("twin", b, dz))
        ref = whole[b].at[pl.ds(0, NX * SHARD), :]
        remote(ref, ref, twin_sem.at[b], twin_arrive.at[b, DZ_ORDER.index(dz)], twin).wait_recv()

    up_load.wait()
    work(0.0)
    for load in (k_load, v_load, docs_load):
        load.wait()

    last = pl.ds(TOK - REACH, REACH)
    docs_band[:, REACH:] = docs_ref[...].reshape(1, TOK).astype(jnp.float32)
    halo = [
        remote(k_ref.at[:, last], k_prev, halo_send.at[0], halo_sem.at[0], line(1)),
        remote(v_ref.at[:, last], v_prev, halo_send.at[1], halo_sem.at[1], line(1)),
        remote(docs_ref.at[last], docs_prev, halo_send.at[2], halo_sem.at[2], line(1)),
    ]
    for copy in halo:
        copy.start()
    clock.send("halo", 2 * HEAD * REACH * 2, "halo", RATE, 2 * LATENCY)

    own_row = pl.multiple_of(place(z, x, c) * SHARD, SHARD)
    up_all[pl.ds(own_row, SHARD), :] = up_ref[...]

    k_band[:, REACH:] = k_ref[...]
    v_band[:, REACH:] = v_ref[...]
    down_load.wait()
    down_all[pl.ds(own_row, SHARD), :] = down_ref[...]
    q_load.wait()
    ahead = (
        REACH
        + lax.broadcasted_iota(jnp.int32, (REACH, 2 * REACH), 0)
        - lax.broadcasted_iota(jnp.int32, (REACH, 2 * REACH), 1)
    )
    in_reach = (ahead >= 0) & (ahead < REACH)

    def attend(block):
        rows = pl.ds(block * REACH, REACH)
        band = pl.ds(block * REACH, 2 * REACH)
        keys = k_band[:, band]
        values = v_band[:, band]
        own_docs = docs_band[:, pl.ds((block + 1) * REACH, REACH)]
        own_docs = jnp.transpose(jnp.broadcast_to(own_docs, (REACH, REACH)))
        own_docs = jnp.concatenate([own_docs, own_docs], axis=1)
        visible = in_reach & (own_docs == docs_band[:, band])
        outs = []
        for h in range(4):
            scores = jnp.dot(
                q_ref[rows, pl.ds(h * HEAD, HEAD)], keys, preferred_element_type=jnp.float32
            ) * HEAD ** (-0.5)
            scores = jnp.where(visible, scores, masked_score)
            sink = sink_ref[h]
            top = jnp.maximum(jnp.max(scores, axis=-1, keepdims=True), sink)
            exponent = jnp.where(visible, jnp.exp(scores - top), 0.0)
            total = jnp.exp(sink - top) + jnp.sum(exponent, axis=-1, keepdims=True)
            shares = (exponent / total).astype(jnp.bfloat16)
            outs.append(
                lax.dot_general(
                    shares, values, (((1,), (1,)), ((), ())), preferred_element_type=jnp.float32
                )
            )
        attended[rows, :] = jnp.concatenate(outs, axis=1).astype(jnp.bfloat16)

    def lanes(of):
        return pl.ds(pl.multiple_of(of * 256, 256), 256)

    def hand_over(block):
        for owner, first, rows in PIECES[block]:
            @pl.when(y != owner)
            def _():
                remote(
                    attended.at[pl.ds(owner * OWN + first, rows), :], heads.at[pl.ds(first, rows), lanes(y)],
                    swap_send.at[0], swap_sem.at[y], {"sp": sp, "tp": owner},
                ).start()

    for block in (1, 2, 3):
        attend(block)
        hand_over(block)
        work(0.88)
    hold("halo")
    for copy in halo:
        copy.wait_recv()
    k_band[:, :REACH] = k_prev[...]
    v_band[:, :REACH] = v_prev[...]
    docs_band[:, :REACH] = jnp.where(sp == 0, -1.0, docs_prev[...].reshape(1, REACH).astype(jnp.float32))
    attend(0)
    hand_over(0)
    work(0.88)
    attend(4)
    hand_over(4)
    for by in (1, 3, 2):
        clock.send(("y", 1 if by < 3 else -1), OWN * 256 * 2, ("swap", by))
    heads[:, lanes(y)] = attended[pl.ds(pl.multiple_of(y * OWN, 32), OWN), :]
    work(0.1)
    w_load.wait()
    res_load.wait()
    gain_load.wait()
    for by in (1, 3, 2):
        other = lax.rem(y + by, NY)
        slot = heads.at[:, lanes(other)]
        hold(("swap", by))
        remote(slot, slot, swap_send.at[0], swap_sem.at[other], column(by)).wait_recv()

    def project(n, carry):
        cols = pl.ds(pl.multiple_of(n * 512, 512), 512)
        product = jnp.dot(heads[...], w_ref[:, cols], preferred_element_type=jnp.float32)
        product = product.astype(jnp.bfloat16).astype(jnp.float32)
        mixed[:, cols] = (res_ref[:, cols].astype(jnp.float32) + product).astype(jnp.bfloat16)
        return carry

    for half in range(2):
        lax.fori_loop(2 * half, 2 * half + 2, project, 0)
        work(0.75)

    def norm(h):
        def step(i, carry):
            rows = pl.ds(pl.multiple_of(h * HALF + i * 16, 16), 16)
            widened = mixed[rows, :].astype(jnp.float32)
            scale = lax.rsqrt(jnp.mean(widened * widened, axis=-1, keepdims=True) + epsilon)
            normed[pl.ds(pl.multiple_of((h * NY + y) * HALF + i * 16, 16), 16), :] = (
                widened * scale * gain_ref[...]
            ).astype(jnp.bfloat16)
            return carry

        lax.fori_loop(0, 5, step, 0)

    before, after, across = lax.rem(y + 3, NY), lax.rem(y + 1, NY), lax.rem(y + 2, NY)

    def row_copy(h, of, side, by, slot):
        ref = normed.at[pl.ds(pl.multiple_of((h * NY + of) * HALF, 16), HALF), pl.ds(side * (D // 2), D // 2)]
        return remote(ref, ref, row_send.at[0], row_sem.at[h, slot], column(by))

    def rows_sent(h, of, side, by, slot):
        row_copy(h, of, side, by, slot).start()
        clock.send(("y", by), HALF * D, ("row", h, slot))

    def rows_come(h, of, side, by, slot):
        hold(("row", h, slot))
        row_copy(h, of, side, by, slot).wait_recv()

    def rows_out(h):
        rows_sent(h, y, 0, 1, 0)
        rows_sent(h, y, 1, -1, 3)
        rows_sent(h, y, 1, 1, 1)
        rows_sent(h, y, 0, -1, 2)

    def rows_on(h):
        rows_come(h, before, 0, 1, 0)
        rows_sent(h, before, 0, 1, 4)
        rows_come(h, after, 1, -1, 3)
        rows_sent(h, after, 1, -1, 5)

    def rows_in(h):
        rows_come(h, before, 1, 1, 1)
        rows_come(h, after, 0, -1, 2)
        rows_come(h, across, 0, 1, 4)
        rows_come(h, across, 1, -1, 5)

    norm(0)
    rows_out(0)
    norm(1)
    work(0.4)
    rows_on(0)
    rows_out(1)
    rows_in(0)
    rows_on(1)
    for dz in DZ_ORDER:
        weights(0, dz)

    def expand(h, begin, end):
        rows = pl.ds(h * NY * HALF, NY * HALF)

        def step(n):
            cols = pl.ds(n * 512, 512)
            before_act = jnp.dot(normed[rows, :], up_all[:, cols], preferred_element_type=jnp.float32)
            hidden[rows, cols] = jnp.square(jnp.maximum(before_act, 0.0)).astype(jnp.bfloat16)

        for n in range(begin, end):
            step(n)
            work(0.8)

    def owner_rows(of):
        return pl.ds(pl.multiple_of(of * HALF, 16), HALF)

    side_a, side_b = pl.ds(0, 128), pl.ds(128, 128)
    there = set()

    def contract(h, i):
        dz = DZ_ORDER[i]
        k = h * 8 + i
        if dz not in there:
            weights(1, dz)
            there.add(dz)
        zz = lax.rem(z - dz + 2 * NZ, NZ)
        parts[k] = lax.dot_general(
            hidden[pl.ds(h * NY * HALF, NY * HALF), :], down_all[pl.ds(pl.multiple_of(zz * 256, 256), 256), :],
            (((1,), (1,)), ((), ())), preferred_element_type=jnp.float32,
        ).astype(jnp.bfloat16)
        remote(parts.at[k, owner_rows(across), side_a], first_a.at[k], sum_send.at[0], sum_sem.at[k, 0],
               column(1)).start()
        remote(parts.at[k, owner_rows(across), side_b], first_b.at[k], sum_send.at[0], sum_sem.at[k, 1],
               column(-1)).start()
        work(0.45)
        clock.send(("y", 1), HALF * 256, ("sum", k, 0))
        clock.send(("y", -1), HALF * 256, ("sum", k, 1))

    def add_and_send(h, i):
        k = h * 8 + i
        for way, (first, final, side, to, by) in enumerate((
            (first_a, last_a, side_a, after, 1), (first_b, last_b, side_b, before, -1),
        )):
            ref = first.at[k]
            hold(("sum", k, way))
            remote(ref, ref, sum_send.at[0], sum_sem.at[k, way], column(by)).wait_recv()
            rows = owner_rows(to)
            parts[k, rows, side] = (
                parts[k, rows, side].astype(jnp.float32) + first[k].astype(jnp.float32)
            ).astype(jnp.bfloat16)
            remote(parts.at[k, rows, :], final.at[k], sum_send.at[0], end_sem.at[k, way], column(by)).start()
            clock.now += 0.03
            clock.send(("y", by), HALF * 512, ("end", k, way))

    def finish(h, i):
        k = h * 8 + i
        zz = lax.rem(z - DZ_ORDER[i] + 2 * NZ, NZ)
        for way, final in enumerate((last_a, last_b)):
            ref = final.at[k]
            hold(("end", k, way))
            remote(ref, ref, sum_send.at[0], end_sem.at[k, way], column(1)).wait_recv()
        branch = (
            parts[k, owner_rows(y), :].astype(jnp.float32)
            + last_a[k].astype(jnp.float32)
            + last_b[k].astype(jnp.float32)
        )
        branch = branch.astype(jnp.bfloat16).astype(jnp.float32)
        rows = pl.ds(h * HALF, HALF)
        out_ref[rows, lanes(zz)] = (mixed[rows, lanes(zz)].astype(jnp.float32) + branch).astype(jnp.bfloat16)
        pltpu.make_async_copy(out_ref.at[rows, lanes(zz)], out_hbm.at[rows, lanes(zz)], out_sem.at[0]).start()

    expand(0, 0, 4)
    contract(*ITEMS[0])
    rows_in(1)
    expand(1, 0, 4)
    for n in range(1, len(ITEMS)):
        contract(*ITEMS[n])
        if n >= LAG:
            add_and_send(*ITEMS[n - LAG])
    for n in range(len(ITEMS) - LAG, len(ITEMS)):
        add_and_send(*ITEMS[n])
    for item in ITEMS:
        finish(*item)
    assert not clock.coming

    for b in range(2):
        ref = whole[b].at[pl.ds(0, 31 * SHARD), :]
        remote(ref, ref, send_sems.at[b], arrive.at[0], twin).wait_send()
        ref = whole[b].at[pl.ds(0, 32 * SHARD), :]
        remote(ref, ref, twin_sem.at[b], arrive.at[0], twin).wait_send()
    for copy in halo:
        copy.wait_send()
    ref = attended.at[pl.ds(0, 3 * OWN), :]
    remote(ref, ref, swap_send.at[0], arrive.at[0], twin).wait_send()
    ref = normed.at[pl.ds(0, 3 * OWN), :]
    remote(ref, ref, row_send.at[0], arrive.at[0], twin).wait_send()
    ref = parts.at[:, pl.ds(0, 3 * HALF), :]
    remote(ref, ref, sum_send.at[0], arrive.at[0], twin).wait_send()
    pltpu.make_async_copy(out_ref, out_hbm, out_sem.at[0]).wait()


def body(
    queries, keys, values, documents, sinks, out_weight, residual, norm_gain, up_weight, down_weight
):
    anywhere = pl.BlockSpec(memory_space=pl.ANY)
    bf16 = jnp.bfloat16
    dma = pltpu.SemaphoreType.DMA
    blocks = len(DZ_ORDER)
    return pl.pallas_call(
        kernel,
        out_shape=jax.ShapeDtypeStruct((OWN, D), bf16),
        in_specs=[anywhere] * 4 + [pl.BlockSpec(memory_space=pltpu.SMEM)] + [anywhere] * 5,
        out_specs=anywhere,
        scratch_shapes=[
            pltpu.VMEM((D, D), bf16),
            pltpu.VMEM((D, D), bf16),
            pltpu.VMEM((1024, D), bf16),
            pltpu.VMEM((OWN, D), bf16),
            pltpu.VMEM((TOK, 256), bf16),
            pltpu.VMEM((HEAD, TOK), bf16),
            pltpu.VMEM((HEAD, TOK), bf16),
            pltpu.VMEM((TOK,), jnp.int32),
            pltpu.VMEM((1, D), jnp.float32),
            pltpu.VMEM((SHARD, D), bf16),
            pltpu.VMEM((SHARD, D), bf16),
            pltpu.VMEM((HEAD, TOK + REACH), bf16),
            pltpu.VMEM((HEAD, TOK + REACH), bf16),
            pltpu.VMEM((HEAD, REACH), bf16),
            pltpu.VMEM((HEAD, REACH), bf16),
            pltpu.VMEM((REACH,), jnp.int32),
            pltpu.VMEM((1, TOK + REACH), jnp.float32),
            pltpu.VMEM((TOK, 256), bf16),
            pltpu.VMEM((OWN, 1024), bf16),
            pltpu.VMEM((OWN, D), bf16),
            pltpu.VMEM((TOK, D), bf16),
            pltpu.VMEM((TOK, D), bf16),
            pltpu.VMEM((2 * blocks, NY * HALF, 256), bf16),
            pltpu.VMEM((2 * blocks, HALF, 128), bf16),
            pltpu.VMEM((2 * blocks, HALF, 128), bf16),
            pltpu.VMEM((2 * blocks, HALF, 256), bf16),
            pltpu.VMEM((2 * blocks, HALF, 256), bf16),
            pltpu.VMEM((OWN, D), bf16),
            dma((len(SLOT),)),
            dma((2,)),
            dma((2,)),
            dma((2, blocks)),
            dma((9,)),
            dma((3,)),
            dma((3,)),
            dma((NY,)),
            dma((1,)),
            dma((2, 6)),
            dma((1,)),
            dma((2 * blocks, 2)),
            dma((1,)),
            dma((2 * blocks, 2)),
            dma((1,)),
        ],
        compiler_params=pltpu.CompilerParams(
            collective_id=0, has_side_effects=True, vmem_limit_bytes=60 * 1024 * 1024
        ),
    )(
        queries, keys.T, values.T, documents, sinks, out_weight, residual,
        norm_gain.reshape(1, D), up_weight, down_weight.T,
    )


def solution(mesh):
    in_specs = (
        P("sp", "tp"),
        P("sp", "tp"),
        P("sp", "tp"),
        P("sp"),
        P("tp"),
        P(),
        P(("sp", "tp"), None),
        P(),
        P("sp", "tp"),
        P("tp", "sp"),
    )
    out_specs = P(("sp", "tp"), None)
    return jax.shard_map(body, mesh=mesh, in_specs=in_specs, out_specs=out_specs, check_vma=False)
```

```python
import functools
import heapq

import jax
import jax.numpy as jnp
from jax import lax
from jax.experimental import pallas as pl
from jax.experimental.pallas import tpu as pltpu
from jax.sharding import PartitionSpec as P

MESH = pl.DeviceIdType.MESH
NZ, NX, NY = 8, 4, 4
HEAD = 64
REACH = 128
TOK = 640
OWN = 160
HALF = 80
D = 2048
SHARD = 32
masked_score = -1e30
epsilon = 1e-06

CUT = 1280
STREAMS = ((0, "z", 0, CUT), (0, "x", CUT, D - CUT), (1, "z", 0, 1152), (1, "x", 1152, D - 1152))
BEGIN = (0.0, 0.0, 20.0, 16.0)
RATE = 46.6e3
LATENCY = 1.8
TWIN_RATE = 600e3
TWIN_LATENCY = 1.0
ISSUE = 0.015
MARGIN = 0.3
LAG = 3
DZ_ORDER = (0, 1, -1, 2, -2, 3, -3, 4)


def onward(item):
    s, dz, dx, part = item
    mode = STREAMS[s][1]
    out = []

    def along_z():
        if dz == 0:
            out.append(("z", 1, (s, 1, dx, None)))
            out.append(("z", -1, (s, -1, dx, None)))
        elif dz in (1, 2):
            out.append(("z", 1, (s, dz + 1, dx, None)))
        elif dz in (-1, -2):
            out.append(("z", -1, (s, dz - 1, dx, None)))
        elif dz == 3:
            out.append(("z", 1, (s, 4, dx, 0)))
        elif dz == -3:
            out.append(("z", -1, (s, 4, dx, 1)))

    def along_x():
        if dx == 0:
            out.append(("x", 1, (s, dz, 1, part)))
            out.append(("x", -1, (s, dz, -1, part)))
        elif dx == 1:
            if dz == 0:
                out.append(("x", 1, (s, dz, 2, 0)))
            elif dz in (1, -2, 3) or (dz == 4 and part == 0):
                out.append(("x", 1, (s, dz, 2, part)))
        elif dx == -1:
            if dz == 0:
                out.append(("x", -1, (s, dz, 2, 1)))
            elif dz in (-1, 2, -3) or (dz == 4 and part == 1):
                out.append(("x", -1, (s, dz, 2, part)))

    if mode == "z":
        if dx == 0:
            along_z()
        along_x()
    else:
        if dz == 0:
            along_x()
        if part is None or dz != 0:
            if part is None:
                along_z()
        elif part == 1:
            along_z()
    return out


def size(item):
    return SHARD * STREAMS[item[0]][3] * 2 // (1 if item[3] is None else 2)


def arrivals():
    found, items = [(s, 0, 0, None) for s in range(len(STREAMS))], []
    while found:
        for _, _, there in onward(found.pop()):
            items.append(there)
            found.append(there)
    return sorted(items, key=str)


SLOT = {item: k for k, item in enumerate(arrivals())}


class Clock:
    def __init__(self):
        self.now = 0.0
        self.free = {}
        self.due = {}
        self.coming = []
        for s, begin in enumerate(BEGIN):
            item = (s, 0, 0, None)
            heapq.heappush(self.coming, (begin, str(item), item))

    def send(self, link, count, label, rate=RATE, latency=LATENCY):
        self.now += ISSUE
        end = max(self.now, self.free.get(link, 0.0)) + count / rate
        self.free[link] = end
        self.due[label] = max(self.due.get(label, 0.0), end + latency)

    def expect(self, item):
        heapq.heappush(self.coming, (self.due[item] + MARGIN, str(item), item))


PIECES = {
    0: ((0, 0, 128),),
    1: ((0, 128, 32), (1, 0, 96)),
    2: ((1, 96, 64), (2, 0, 64)),
    3: ((2, 64, 96), (3, 0, 32)),
    4: ((3, 32, 128),),
}
ITEMS = ((0, 0),) + tuple((h, i) for i in range(8) for h in range(2) if (h, i) != (0, 0))


def kernel(
    q_hbm, k_hbm, v_hbm, docs_hbm, sink_ref, w_hbm, res_hbm, gain_hbm, up_hbm, down_hbm,
    out_hbm,
    up_all, down_all, w_ref, res_ref, q_ref, k_ref, v_ref, docs_ref, gain_ref, up_ref, down_ref,
    k_band, v_band, k_prev, v_prev, docs_prev, docs_band,
    attended, heads, mixed, normed, hidden, parts, first_a, first_b, last_a, last_b, out_ref,
    arrive, send_sems, twin_sem, twin_arrive, load_sem, halo_sem, halo_send,
    swap_sem, swap_send, row_sem, row_send, sum_sem, sum_send, end_sem, out_sem,
):
    sp = lax.axis_index("sp")
    y = lax.axis_index("tp")
    c = lax.rem(sp, 2)
    x = lax.rem(sp // 2, NX)
    z = sp // (2 * NX)

    def place(zz, xx, cc):
        return (zz * NX + xx) * 2 + cc

    def near(axis, way):
        if axis == "z":
            return {"sp": place(lax.rem(z + way + NZ, NZ), x, c), "tp": y}
        return {"sp": place(z, lax.rem(x + way + NX, NX), c), "tp": y}

    twin = {"sp": place(z, x, 1 - c), "tp": y}

    def column(by):
        return {"sp": sp, "tp": lax.rem(y + by + NY, NY)}

    def line(by):
        return {"sp": lax.rem(sp + by + 2 * NX * NZ, 2 * NX * NZ), "tp": y}

    up_load, down_load, k_load, v_load, docs_load, q_load, gain_load, res_load, w_load = loads = [
        pltpu.make_async_copy(src, dst, load_sem.at[n])
        for n, (src, dst) in enumerate((
            (up_hbm, up_ref), (down_hbm, down_ref), (k_hbm, k_ref), (v_hbm, v_ref), (docs_hbm, docs_ref),
            (q_hbm, q_ref), (gain_hbm, gain_ref), (res_hbm, res_ref), (w_hbm, w_ref),
        ))
    ]
    for load in loads:
        load.start()

    barrier = pltpu.get_barrier_semaphore()
    greeted = [near("z", 1), near("z", -1), near("x", 1), near("x", -1), twin,
               column(1), column(2), column(3), line(1), line(-1)]
    for device in greeted:
        pl.semaphore_signal(barrier, inc=1, device_id=device, device_id_type=MESH)
    pl.semaphore_wait(barrier, len(greeted))

    def remote(src, dst, send, recv, device):
        return pltpu.make_async_remote_copy(
            src_ref=src, dst_ref=dst, send_sem=send, recv_sem=recv, device_id=device, device_id_type=MESH
        )

    whole = (up_all, down_all)
    shards = (up_ref, down_ref)

    def view(item):
        s, dz, dx, part = item
        b, _, first, count = STREAMS[s]
        zz = lax.rem(z - dz + 2 * NZ, NZ)
        xx = lax.rem(x - dx + 2 * NX, NX)
        row = place(zz, xx, c) * SHARD
        rows = SHARD
        if part is not None:
            rows = SHARD // 2
            row = row + part * rows
        return whole[b].at[pl.ds(pl.multiple_of(row, 16), rows), pl.ds(first, count)]

    def own_view(s, part):
        b, _, first, count = STREAMS[s]
        if part is None:
            return shards[b].at[:, pl.ds(first, count)]
        return shards[b].at[pl.ds(part * (SHARD // 2), SHARD // 2), pl.ds(first, count)]

    clock = Clock()
    halves = set()
    left = {(b, dz): NX * SHARD * D * 2 for b in range(2) for dz in DZ_ORDER}

    def pass_on(item):
        s, dz, dx, part = item
        b = STREAMS[s][0]
        own = dz == 0 and dx == 0
        sent = onward(item)
        if STREAMS[s][1] == "x" and dz == 0 and dx == 2:
            halves.add(item)
            sent = onward((s, 0, 2, 1)) if {(s, 0, 2, 0), (s, 0, 2, 1)} <= halves else []
        for axis, way, there in sent:
            here = (s, dz, dx, there[3])
            src = own_view(s, there[3]) if own else view(here)
            remote(src, view(here), send_sems.at[b], arrive.at[SLOT[there]], near(axis, way)).start()
            clock.send((axis, way), size(there), there)
            clock.expect(there)
        src = own_view(s, part) if own else view(item)
        remote(src, view(item), twin_sem.at[b], twin_arrive.at[b, DZ_ORDER.index(dz)], twin).start()
        clock.send("twin", size(item), ("twin", b, dz), TWIN_RATE, TWIN_LATENCY)
        left[b, dz] -= size(item)

    def take():
        moment, _, item = heapq.heappop(clock.coming)
        clock.now = max(clock.now, moment)
        if item[1] != 0 or item[2] != 0:
            ref = view(item)
            remote(ref, ref, send_sems.at[0], arrive.at[SLOT[item]], twin).wait_recv()
        pass_on(item)

    def work(us):
        clock.now += us
        while clock.coming and clock.coming[0][0] <= clock.now:
            take()

    def hold(label):
        while clock.coming and clock.coming[0][0] < clock.due[label]:
            take()
        clock.now = max(clock.now, clock.due[label])

    def weights(b, dz):
        while left[b, dz] > 0:
            take()
        hold(("twin", b, dz))
        ref = whole[b].at[pl.ds(0, NX * SHARD), :]
        remote(ref, ref, twin_sem.at[b], twin_arrive.at[b, DZ_ORDER.index(dz)], twin).wait_recv()

    up_load.wait()
    work(0.0)
    for load in (k_load, v_load, docs_load):
        load.wait()

    last = pl.ds(TOK - REACH, REACH)
    docs_band[:, REACH:] = docs_ref[...].reshape(1, TOK).astype(jnp.float32)
    halo = [
        remote(k_ref.at[:, last], k_prev, halo_send.at[0], halo_sem.at[0], line(1)),
        remote(v_ref.at[:, last], v_prev, halo_send.at[1], halo_sem.at[1], line(1)),
        remote(docs_ref.at[last], docs_prev, halo_send.at[2], halo_sem.at[2], line(1)),
    ]
    for copy in halo:
        copy.start()
    clock.send("halo", 2 * HEAD * REACH * 2, "halo", RATE, 2 * LATENCY)

    own_row = pl.multiple_of(place(z, x, c) * SHARD, SHARD)
    up_all[pl.ds(own_row, SHARD), :] = up_ref[...]

    k_band[:, REACH:] = k_ref[...]
    v_band[:, REACH:] = v_ref[...]
    down_load.wait()
    down_all[pl.ds(own_row, SHARD), :] = down_ref[...]
    q_load.wait()
    ahead = (
        REACH
        + lax.broadcasted_iota(jnp.int32, (REACH, 2 * REACH), 0)
        - lax.broadcasted_iota(jnp.int32, (REACH, 2 * REACH), 1)
    )
    in_reach = (ahead >= 0) & (ahead < REACH)

    def attend(block):
        rows = pl.ds(block * REACH, REACH)
        band = pl.ds(block * REACH, 2 * REACH)
        keys = k_band[:, band]
        values = v_band[:, band]
        own_docs = docs_band[:, pl.ds((block + 1) * REACH, REACH)]
        own_docs = jnp.transpose(jnp.broadcast_to(own_docs, (REACH, REACH)))
        own_docs = jnp.concatenate([own_docs, own_docs], axis=1)
        visible = in_reach & (own_docs == docs_band[:, band])
        outs = []
        for h in range(4):
            scores = jnp.dot(
                q_ref[rows, pl.ds(h * HEAD, HEAD)], keys, preferred_element_type=jnp.float32
            ) * HEAD ** (-0.5)
            scores = jnp.where(visible, scores, masked_score)
            sink = sink_ref[h]
            top = jnp.maximum(jnp.max(scores, axis=-1, keepdims=True), sink)
            exponent = jnp.where(visible, jnp.exp(scores - top), 0.0)
            total = jnp.exp(sink - top) + jnp.sum(exponent, axis=-1, keepdims=True)
            shares = (exponent / total).astype(jnp.bfloat16)
            outs.append(
                lax.dot_general(
                    shares, values, (((1,), (1,)), ((), ())), preferred_element_type=jnp.float32
                )
            )
        attended[rows, :] = jnp.concatenate(outs, axis=1).astype(jnp.bfloat16)

    def lanes(of):
        return pl.ds(pl.multiple_of(of * 256, 256), 256)

    def hand_over(block):
        for owner, first, rows in PIECES[block]:
            @pl.when(y != owner)
            def _():
                remote(
                    attended.at[pl.ds(owner * OWN + first, rows), :], heads.at[pl.ds(first, rows), lanes(y)],
                    swap_send.at[0], swap_sem.at[y], {"sp": sp, "tp": owner},
                ).start()

    for block in (1, 2, 3):
        attend(block)
        hand_over(block)
        work(0.88)
    hold("halo")
    for copy in halo:
        copy.wait_recv()
    k_band[:, :REACH] = k_prev[...]
    v_band[:, :REACH] = v_prev[...]
    docs_band[:, :REACH] = jnp.where(sp == 0, -1.0, docs_prev[...].reshape(1, REACH).astype(jnp.float32))
    attend(0)
    hand_over(0)
    work(0.88)
    attend(4)
    hand_over(4)
    for by in (1, 3, 2):
        clock.send(("y", 1 if by < 3 else -1), OWN * 256 * 2, ("swap", by))
    heads[:, lanes(y)] = attended[pl.ds(pl.multiple_of(y * OWN, 32), OWN), :]
    work(0.1)
    w_load.wait()
    res_load.wait()
    gain_load.wait()
    for by in (1, 3, 2):
        other = lax.rem(y + by, NY)
        slot = heads.at[:, lanes(other)]
        hold(("swap", by))
        remote(slot, slot, swap_send.at[0], swap_sem.at[other], column(by)).wait_recv()

    def project(n, carry):
        cols = pl.ds(pl.multiple_of(n * 512, 512), 512)
        product = jnp.dot(heads[...], w_ref[:, cols], preferred_element_type=jnp.float32)
        product = product.astype(jnp.bfloat16).astype(jnp.float32)
        mixed[:, cols] = (res_ref[:, cols].astype(jnp.float32) + product).astype(jnp.bfloat16)
        return carry

    for half in range(2):
        lax.fori_loop(2 * half, 2 * half + 2, project, 0)
        work(0.75)

    def norm(h):
        def step(i, carry):
            rows = pl.ds(pl.multiple_of(h * HALF + i * 16, 16), 16)
            widened = mixed[rows, :].astype(jnp.float32)
            scale = lax.rsqrt(jnp.mean(widened * widened, axis=-1, keepdims=True) + epsilon)
            normed[pl.ds(pl.multiple_of((h * NY + y) * HALF + i * 16, 16), 16), :] = (
                widened * scale * gain_ref[...]
            ).astype(jnp.bfloat16)
            return carry

        lax.fori_loop(0, 5, step, 0)

    before, after, across = lax.rem(y + 3, NY), lax.rem(y + 1, NY), lax.rem(y + 2, NY)

    def row_copy(h, of, side, by, slot):
        ref = normed.at[pl.ds(pl.multiple_of((h * NY + of) * HALF, 16), HALF), pl.ds(side * (D // 2), D // 2)]
        return remote(ref, ref, row_send.at[0], row_sem.at[h, slot], column(by))

    def rows_sent(h, of, side, by, slot):
        row_copy(h, of, side, by, slot).start()
        clock.send(("y", by), HALF * D, ("row", h, slot))

    def rows_come(h, of, side, by, slot):
        hold(("row", h, slot))
        row_copy(h, of, side, by, slot).wait_recv()

    def rows_out(h):
        rows_sent(h, y, 0, 1, 0)
        rows_sent(h, y, 1, -1, 3)
        rows_sent(h, y, 1, 1, 1)
        rows_sent(h, y, 0, -1, 2)

    def rows_on(h):
        rows_come(h, before, 0, 1, 0)
        rows_sent(h, before, 0, 1, 4)
        rows_come(h, after, 1, -1, 3)
        rows_sent(h, after, 1, -1, 5)

    def rows_in(h):
        rows_come(h, before, 1, 1, 1)
        rows_come(h, after, 0, -1, 2)
        rows_come(h, across, 0, 1, 4)
        rows_come(h, across, 1, -1, 5)

    norm(0)
    rows_out(0)
    norm(1)
    work(0.4)
    rows_on(0)
    rows_out(1)
    rows_in(0)
    rows_on(1)
    for dz in DZ_ORDER:
        weights(0, dz)

    def expand(h, begin, end):
        rows = pl.ds(h * NY * HALF, NY * HALF)

        def step(n):
            cols = pl.ds(n * 512, 512)
            before_act = jnp.dot(normed[rows, :], up_all[:, cols], preferred_element_type=jnp.float32)
            hidden[rows, cols] = jnp.square(jnp.maximum(before_act, 0.0)).astype(jnp.bfloat16)

        for n in range(begin, end):
            step(n)
            work(0.8)

    def owner_rows(of):
        return pl.ds(pl.multiple_of(of * HALF, 16), HALF)

    side_a, side_b = pl.ds(0, 128), pl.ds(128, 128)
    there = set()

    def contract(h, i):
        dz = DZ_ORDER[i]
        k = h * 8 + i
        if dz not in there:
            weights(1, dz)
            there.add(dz)
        zz = lax.rem(z - dz + 2 * NZ, NZ)
        parts[k] = lax.dot_general(
            hidden[pl.ds(h * NY * HALF, NY * HALF), :], down_all[pl.ds(pl.multiple_of(zz * 256, 256), 256), :],
            (((1,), (1,)), ((), ())), preferred_element_type=jnp.float32,
        ).astype(jnp.bfloat16)
        remote(parts.at[k, owner_rows(across), side_a], first_a.at[k], sum_send.at[0], sum_sem.at[k, 0],
               column(1)).start()
        remote(parts.at[k, owner_rows(across), side_b], first_b.at[k], sum_send.at[0], sum_sem.at[k, 1],
               column(-1)).start()
        work(0.45)
        clock.send(("y", 1), HALF * 256, ("sum", k, 0))
        clock.send(("y", -1), HALF * 256, ("sum", k, 1))

    def add_and_send(h, i):
        k = h * 8 + i
        for way, (first, final, side, to, by) in enumerate((
            (first_a, last_a, side_a, after, 1), (first_b, last_b, side_b, before, -1),
        )):
            ref = first.at[k]
            hold(("sum", k, way))
            remote(ref, ref, sum_send.at[0], sum_sem.at[k, way], column(by)).wait_recv()
            rows = owner_rows(to)
            parts[k, rows, side] = (
                parts[k, rows, side].astype(jnp.float32) + first[k].astype(jnp.float32)
            ).astype(jnp.bfloat16)
            remote(parts.at[k, rows, :], final.at[k], sum_send.at[0], end_sem.at[k, way], column(by)).start()
            clock.now += 0.03
            clock.send(("y", by), HALF * 512, ("end", k, way))

    def finish(h, i):
        k = h * 8 + i
        zz = lax.rem(z - DZ_ORDER[i] + 2 * NZ, NZ)
        for way, final in enumerate((last_a, last_b)):
            ref = final.at[k]
            hold(("end", k, way))
            remote(ref, ref, sum_send.at[0], end_sem.at[k, way], column(1)).wait_recv()
        branch = (
            parts[k, owner_rows(y), :].astype(jnp.float32)
            + last_a[k].astype(jnp.float32)
            + last_b[k].astype(jnp.float32)
        )
        branch = branch.astype(jnp.bfloat16).astype(jnp.float32)
        rows = pl.ds(h * HALF, HALF)
        out_ref[rows, lanes(zz)] = (mixed[rows, lanes(zz)].astype(jnp.float32) + branch).astype(jnp.bfloat16)
        pltpu.make_async_copy(out_ref.at[rows, lanes(zz)], out_hbm.at[rows, lanes(zz)], out_sem.at[0]).start()

    expand(0, 0, 4)
    contract(*ITEMS[0])
    rows_in(1)
    expand(1, 0, 4)
    for n in range(1, len(ITEMS)):
        contract(*ITEMS[n])
        if n >= LAG:
            add_and_send(*ITEMS[n - LAG])
    for n in range(len(ITEMS) - LAG, len(ITEMS)):
        add_and_send(*ITEMS[n])
    for item in ITEMS:
        finish(*item)
    assert not clock.coming

    for b in range(2):
        ref = whole[b].at[pl.ds(0, 31 * SHARD), :]
        remote(ref, ref, send_sems.at[b], arrive.at[0], twin).wait_send()
        ref = whole[b].at[pl.ds(0, 32 * SHARD), :]
        remote(ref, ref, twin_sem.at[b], arrive.at[0], twin).wait_send()
    for copy in halo:
        copy.wait_send()
    ref = attended.at[pl.ds(0, 3 * OWN), :]
    remote(ref, ref, swap_send.at[0], arrive.at[0], twin).wait_send()
    ref = normed.at[pl.ds(0, 3 * OWN), :]
    remote(ref, ref, row_send.at[0], arrive.at[0], twin).wait_send()
    ref = parts.at[:, pl.ds(0, 3 * HALF), :]
    remote(ref, ref, sum_send.at[0], arrive.at[0], twin).wait_send()
    pltpu.make_async_copy(out_ref, out_hbm, out_sem.at[0]).wait()


def body(
    queries, keys, values, documents, sinks, out_weight, residual, norm_gain, up_weight, down_weight
):
    anywhere = pl.BlockSpec(memory_space=pl.ANY)
    bf16 = jnp.bfloat16
    dma = pltpu.SemaphoreType.DMA
    blocks = len(DZ_ORDER)
    return pl.pallas_call(
        kernel,
        out_shape=jax.ShapeDtypeStruct((OWN, D), bf16),
        in_specs=[anywhere] * 4 + [pl.BlockSpec(memory_space=pltpu.SMEM)] + [anywhere] * 5,
        out_specs=anywhere,
        scratch_shapes=[
            pltpu.VMEM((D, D), bf16),
            pltpu.VMEM((D, D), bf16),
            pltpu.VMEM((1024, D), bf16),
            pltpu.VMEM((OWN, D), bf16),
            pltpu.VMEM((TOK, 256), bf16),
            pltpu.VMEM((HEAD, TOK), bf16),
            pltpu.VMEM((HEAD, TOK), bf16),
            pltpu.VMEM((TOK,), jnp.int32),
            pltpu.VMEM((1, D), jnp.float32),
            pltpu.VMEM((SHARD, D), bf16),
            pltpu.VMEM((SHARD, D), bf16),
            pltpu.VMEM((HEAD, TOK + REACH), bf16),
            pltpu.VMEM((HEAD, TOK + REACH), bf16),
            pltpu.VMEM((HEAD, REACH), bf16),
            pltpu.VMEM((HEAD, REACH), bf16),
            pltpu.VMEM((REACH,), jnp.int32),
            pltpu.VMEM((1, TOK + REACH), jnp.float32),
            pltpu.VMEM((TOK, 256), bf16),
            pltpu.VMEM((OWN, 1024), bf16),
            pltpu.VMEM((OWN, D), bf16),
            pltpu.VMEM((TOK, D), bf16),
            pltpu.VMEM((TOK, D), bf16),
            pltpu.VMEM((2 * blocks, NY * HALF, 256), bf16),
            pltpu.VMEM((2 * blocks, HALF, 128), bf16),
            pltpu.VMEM((2 * blocks, HALF, 128), bf16),
            pltpu.VMEM((2 * blocks, HALF, 256), bf16),
            pltpu.VMEM((2 * blocks, HALF, 256), bf16),
            pltpu.VMEM((OWN, D), bf16),
            dma((len(SLOT),)),
            dma((2,)),
            dma((2,)),
            dma((2, blocks)),
            dma((9,)),
            dma((3,)),
            dma((3,)),
            dma((NY,)),
            dma((1,)),
            dma((2, 6)),
            dma((1,)),
            dma((2 * blocks, 2)),
            dma((1,)),
            dma((2 * blocks, 2)),
            dma((1,)),
        ],
        compiler_params=pltpu.CompilerParams(
            collective_id=0, has_side_effects=True, vmem_limit_bytes=60 * 1024 * 1024
        ),
    )(
        queries, keys.T, values.T, documents, sinks, out_weight, residual,
        norm_gain.reshape(1, D), up_weight, down_weight.T,
    )


def solution(mesh):
    in_specs = (
        P("sp", "tp"),
        P("sp", "tp"),
        P("sp", "tp"),
        P("sp"),
        P("tp"),
        P(),
        P(("sp", "tp"), None),
        P(),
        P("sp", "tp"),
        P("tp", "sp"),
    )
    out_specs = P(("sp", "tp"), None)
    return jax.shard_map(body, mesh=mesh, in_specs=in_specs, out_specs=out_specs, check_vma=False)
```
